32 devices in a mesh: sp: 16 (over z, y, x), tp: 2 (over core).
Axes of the slice: x: 2, y: 2, z: 4, core: 2. Of those that a mesh axis runs over, the one named last changes fastest.
Arguments:
- mid_stream: bfloat16 [5120, 2048], P('sp', 'tp'), may hold values from -6 to 6
- layer_cot: bfloat16 [5120, 2048], P('sp', 'tp'), may hold values from -6 to 6
- ffn_gain: bfloat16 [2048], P('tp'), may hold values from 0.099609375 to 1.8984375
- expert_ids: int32 [5120, 2], P('sp'), may hold values from 0 to 15, all different within a row; in each aligned block of 320 rows (0 to 319, 320 to 639, ...) at most 80 rows name the same one
- group_prob: float32 [5120], P('sp'), may hold values from 0.25 to 1
- first_share: float32 [5120], P('sp'), may hold values from 0.5 to 0.95
- expert_gate: bfloat16 [16, 2048, 1024], P('sp', None, 'tp'), may hold values from -0.125 to 0.125
- expert_up: bfloat16 [16, 2048, 1024], P('sp', None, 'tp'), may hold values from -0.125 to 0.125
- expert_down: bfloat16 [16, 1024, 2048], P('sp', 'tp'), may hold values from -0.1875 to 0.1875
- out_weight: bfloat16 [2048, 1024], P(None, 'tp'), may hold values from -0.1875 to 0.1875
- conv_gain: bfloat16 [1024], P('tp'), may hold values from 0.099609375 to 1.8984375
- b_gate: bfloat16 [5120, 1024], P('sp', 'tp'), may hold values from -6 to 6
- c_gate: bfloat16 [5120, 1024], P('sp', 'tp'), may hold values from -6 to 6
- conv_in: bfloat16 [5120, 1024], P('sp', 'tp'), may hold values from -6 to 6
- conv_out: bfloat16 [5120, 1024], P('sp', 'tp'), may hold values from -6 to 6
- conv_taps: bfloat16 [3, 1024], P(None, 'tp'), may hold values from -3.5 to 3.5
Outputs:
- grad_gate: float32 [16, 2048, 1024], P('sp', None, 'tp')
- grad_up: float32 [16, 2048, 1024], P('sp', None, 'tp')
- grad_down: float32 [16, 1024, 2048], P('sp', 'tp')
- grad_out_weight: float32 [2048, 1024], P('sp', 'tp')
- mid_grad: bfloat16 [5120, 2048], P('sp', 'tp')
- grad_b: bfloat16 [5120, 1024], P('sp', 'tp')
- grad_c: bfloat16 [5120, 1024], P('sp', 'tp')
- grad_conv_in: bfloat16 [5120, 1024], P('sp', 'tp')
The draws below stay inside these ranges and needn't reach their ends.
Inputs may be any that keep to these rules, and one draw needn't show every extreme that they name: `expert_ids`: each row names 2 different experts. Among the rows of one device no expert is named more than 80 times, a bound that some block reaches.
All inputs are finite; a program needn't handle non-finite values.
Results may differ from the reference program's by a relative error of at most 0.0067.
Values may be sent and summed in bfloat16 or wider, within the bound.
A program may use at most 128 MiB of HBM per device.

```python
import math
import jax
import jax.numpy as jnp
import numpy as np
from jax import lax

D = 2048
CONV_CH = 1024
GROUP = 64
FF = 1024
TOP = 2
TOK_DEV = 320
TOKENS = 5120
EXPERTS = 16
CAP = 80
N_SP = 16
N_TP = 2


def with_spikes(entries, key, source, target, parts, factor):
    def block_of(position):
        return (jnp.arange(entries.shape[position]) // (entries.shape[position] // parts)).reshape((-1,) + (1,) * (entries.ndim - 1 - position))

    first = jax.random.permutation(key, parts)[block_of(target)]
    far = (block_of(target) + parts // 2) % parts
    return jnp.where((block_of(source) == first) | (block_of(source) == far), factor * entries, entries)


def block_scale(rng, dims, shards, least, high):
    gain, own = 1.0, jax.random.fold_in(rng, 6)
    for dim, blocks in shards:
        draws = jnp.exp(jax.random.uniform(jax.random.fold_in(own, dim), (blocks,), jnp.float32, least / len(shards), high / len(shards)))
        gain = gain * jnp.repeat(draws, dims[dim] // blocks).reshape([-1 if axis == dim else 1 for axis in range(len(dims))])
    return gain


def shared_out(stream_key, own, number, rows, number_of, top, limit, skew):
    order = jax.random.permutation(stream_key, number_of)
    crowded, ordinary = portions_of(number_of, rows * top, limit, skew, True), portions_of(number_of, rows * top, limit, skew, False)
    places = jnp.arange(number_of)

    def named(lengths, offset_by):
        used = int((lengths > 0).sum())
        fixed = max(1, used // 4)
        moved = fixed + (places - fixed + offset_by * (used - fixed)) % max(1, number_of - fixed)
        return jnp.zeros((number_of,), jnp.int32).at[order[jnp.where(places < fixed, places, moved)]].set(jnp.asarray(lengths, jnp.int32))

    lengths = jnp.where(number % 4 == 0, named(crowded, number // 4), named(ordinary, number - number // 4 - 1))
    mixed = jax.random.permutation(jax.random.fold_in(own, 3), number_of)
    source_of, taker = mixed[0:number_of // 2 * 2:2], mixed[1:number_of // 2 * 2:2]
    slack = jnp.minimum(lengths[source_of] - 1, limit - lengths[taker]) // 2
    slack = jnp.where((source_of == order[0]) | (taker == order[0]) | (lengths[taker] == 0), 0, jnp.maximum(slack, 0))
    moved = jax.random.randint(jax.random.fold_in(own, 4), (number_of // 2,), 0, 1 << 20) % (slack + 1)
    lengths = lengths.at[source_of].add(-moved).at[taker].add(moved)
    items = jnp.searchsorted(jnp.cumsum(lengths), jnp.arange(rows * top), side="right").astype(jnp.int32)
    table = items.reshape(top, rows).T
    table = table[jax.random.permutation(jax.random.fold_in(own, 1), rows)]
    offset_by = jax.random.randint(jax.random.fold_in(own, 2), (rows, 1), 0, top)
    return jnp.take_along_axis(table, (jnp.arange(top)[None, :] + offset_by) % top, axis=1)


def portions_of(amount, total, limit, skew, full):
    loads = [(1 << 20) // math.isqrt(rank ** skew) + 1 for rank in range(1, amount + 1)]
    largest = limit if full else min(limit, max(-(-total // amount), total * loads[0] // sum(loads)))
    least = 1 if total - largest >= amount - 1 else 0
    given, rest = [largest] + [least] * (amount - 1), total - largest - least * (amount - 1)
    while rest > 0:
        free = [i for i in range(1, amount) if given[i] < largest] or [i for i in range(1, amount) if given[i] < limit]
        pool, remaining = sum([loads[i] for i in free]), rest
        for i in free:
            addition = min(limit - given[i], max(1, remaining * loads[i] // pool), rest)
            given[i] = given[i] + addition
            rest = rest - addition
    return np.array(given)


def bell_draw(key, extent, width, limit, shards=(), held_as=jnp.bfloat16):
    values = width * jax.random.normal(key, extent, jnp.float32)
    if shards:
        values = values * block_scale(key, extent, shards, -0.22, 0.18)
    return jnp.clip(values, -limit, limit).astype(held_as)


def bell_draw_with(stream_key, shape, scale, reach, cuts, heavy, kind=jnp.bfloat16):
    result = scale * jax.random.normal(stream_key, shape, jnp.float32)
    if cuts:
        result = result * block_scale(stream_key, shape, cuts, -0.22, 0.18)
    return jnp.clip(with_spikes(result, jax.random.fold_in(stream_key, 3), *heavy), -reach, reach).astype(kind)


def setup_inputs(seed: int = 0) -> dict:
    key_of = jax.random.split(jax.random.key(seed), 17)
    mid_stream = bell_draw(key_of[0], (TOKENS, D), 1.0, 6.0, ((0, 16), (1, 2)))
    layer_cot = bell_draw_with(key_of[1], (TOKENS, D), 1.0, 6.0, ((0, 16), (1, 2)), (0, 1, 16, 2.0))
    ffn_gain = jnp.clip(1.0 + 0.18 * jax.random.normal(key_of[2], (D,), jnp.float32), 0.099609375, 1.8984375).astype(jnp.bfloat16)
    expert_ids_keys = jax.random.split(jax.random.fold_in(key_of[3], 1), TOKENS // TOK_DEV)
    expert_ids_turns = jax.random.permutation(jax.random.fold_in(key_of[3], 3), TOKENS // TOK_DEV)
    expert_ids = jax.vmap(lambda own, number: shared_out(jax.random.fold_in(key_of[3], 2), own, number, TOK_DEV, EXPERTS, TOP, CAP, 2))(expert_ids_keys, expert_ids_turns).reshape((TOKENS, TOP))
    group_prob = jnp.clip(0.25 + 0.75 * jax.random.uniform(key_of[4], (TOKENS,), jnp.float32) ** block_scale(key_of[4], (TOKENS,), ((0, 16),), -0.2, 0.2), 0.25, 1.0)
    first_share = jnp.clip(0.5 + 0.45 * jax.random.uniform(key_of[5], (TOKENS,), jnp.float32) ** block_scale(key_of[5], (TOKENS,), ((0, 16),), -0.2, 0.2), 0.5, 0.95)
    expert_gate = bell_draw(key_of[6], (EXPERTS, D, FF), D ** -0.5, 0.125, ((0, 16), (2, 2)))
    expert_up = bell_draw(key_of[7], (EXPERTS, D, FF), D ** -0.5, 0.125, ((0, 16), (2, 2)))
    expert_down = bell_draw(key_of[8], (EXPERTS, FF, D), FF ** -0.5, 0.1875, ((0, 16), (1, 2)))
    out_weight = bell_draw(key_of[9], (D, CONV_CH), CONV_CH ** -0.5, 0.1875, ((1, 2),))
    conv_gain = jnp.clip(1.0 + 0.18 * jax.random.normal(key_of[10], (CONV_CH,), jnp.float32), 0.099609375, 1.8984375).astype(jnp.bfloat16)
    b_gate = bell_draw(key_of[11], (TOKENS, CONV_CH), 1.0, 6.0, ((0, 16), (1, 2)))
    c_gate = bell_draw(key_of[12], (TOKENS, CONV_CH), 1.0, 6.0, ((0, 16), (1, 2)))
    conv_in = bell_draw(key_of[13], (TOKENS, CONV_CH), 1.0, 6.0, ((0, 16), (1, 2)))
    conv_out = bell_draw(key_of[14], (TOKENS, CONV_CH), 1.0, 6.0, ((0, 16), (1, 2)))
    conv_taps = bell_draw(key_of[15], (3, CONV_CH), 3 ** -0.5, 3.5, ((1, 2),))
    return dict(mid_stream=mid_stream, layer_cot=layer_cot, ffn_gain=ffn_gain, expert_ids=expert_ids, group_prob=group_prob, first_share=first_share, expert_gate=expert_gate, expert_up=expert_up, expert_down=expert_down, out_weight=out_weight, conv_gain=conv_gain, b_gate=b_gate, c_gate=c_gate, conv_in=conv_in, conv_out=conv_out, conv_taps=conv_taps)


epsilon = 1e-06

def silu_parts(pre):
    sigma = jax.nn.sigmoid(pre)
    return (pre * sigma, sigma * (1.0 + pre * (1.0 - sigma)))

def expert_backward(tokens_in, cots_in, gate_w, up_w, down_w):
    pre_gate = jnp.dot(tokens_in, gate_w, preferred_element_type=jnp.float32)
    pre_up = jnp.dot(tokens_in, up_w, preferred_element_type=jnp.float32)
    active, slope = silu_parts(pre_gate)
    hidden = (active * pre_up).astype(jnp.bfloat16)
    grad_down = jnp.dot(hidden.T, cots_in, preferred_element_type=jnp.float32)
    d_hidden = jnp.dot(cots_in, down_w.T, preferred_element_type=jnp.float32)
    d_gate = (d_hidden * pre_up * slope).astype(jnp.bfloat16)
    d_up = (d_hidden * active).astype(jnp.bfloat16)
    grad_gate = jnp.dot(tokens_in.T, d_gate, preferred_element_type=jnp.float32)
    grad_up = jnp.dot(tokens_in.T, d_up, preferred_element_type=jnp.float32)
    block_width = FF // N_TP
    summed = jnp.zeros((tokens_in.shape[0], D), jnp.float32)
    for block_number in range(N_TP):
        first_col = block_number * block_width
        last_col = first_col + block_width
        partial_term = jnp.dot(d_gate[:, first_col:last_col], gate_w[:, first_col:last_col].T, preferred_element_type=jnp.float32)
        partial_term = partial_term + jnp.dot(d_up[:, first_col:last_col], up_w[:, first_col:last_col].T, preferred_element_type=jnp.float32)
        rounded = lax.optimization_barrier(partial_term.astype(jnp.bfloat16))
        summed = summed + rounded.astype(jnp.float32)
    return (grad_gate, grad_up, grad_down, summed.astype(jnp.bfloat16))

def reference(mid_stream, layer_cot, ffn_gain, expert_ids, group_prob, first_share, expert_gate, expert_up, expert_down, out_weight, conv_gain, b_gate, c_gate, conv_in, conv_out, conv_taps):
    token_count = mid_stream.shape[0]
    mid32 = mid_stream.astype(jnp.float32)
    gain32 = ffn_gain.astype(jnp.float32)
    inv_rms = lax.rsqrt(lax.optimization_barrier(jnp.mean(mid32 * mid32, axis=1)) + epsilon)
    normed = (mid32 * inv_rms[:, None] * gain32).astype(jnp.bfloat16)
    shares = jnp.stack([group_prob * first_share, group_prob * (1.0 - first_share)], axis=1)
    weighted = (layer_cot.astype(jnp.float32)[:, None, :] * shares[:, :, None]).astype(jnp.bfloat16)
    flat_ids = expert_ids.reshape(-1).astype(jnp.int32)
    pair_count = flat_ids.shape[0]
    depth = N_SP * CAP
    onehot = (flat_ids[:, None] == jnp.arange(EXPERTS, dtype=jnp.int32)[None, :]).astype(jnp.int32)
    before = jnp.cumsum(onehot, axis=0) - onehot
    ranks = lax.optimization_barrier(jnp.sum(before * onehot, axis=1)).astype(jnp.int32)
    slot_index = (flat_ids * depth + ranks).astype(jnp.int32)
    source = jnp.full((EXPERTS * depth,), pair_count, jnp.int32)
    source = source.at[slot_index].set(jnp.arange(pair_count, dtype=jnp.int32)).reshape(EXPERTS, depth)
    normed_pad = jnp.concatenate([normed, jnp.zeros((1, D), jnp.bfloat16)], axis=0)
    weighted_pad = jnp.concatenate([weighted.reshape(pair_count, D), jnp.zeros((1, D), jnp.bfloat16)], axis=0)

    def per_expert(packed):
        rows_of, gate_w, up_w, down_w = packed
        tokens_in = normed_pad[rows_of // 2]
        cots_in = weighted_pad[rows_of]
        return expert_backward(tokens_in, cots_in, gate_w, up_w, down_w)
    grad_gate, grad_up, grad_down, back_all = lax.map(per_expert, (source, expert_gate, expert_up, expert_down))
    back_rows = back_all.reshape(EXPERTS * depth, D)[slot_index]
    d_normed = lax.optimization_barrier(jnp.sum(back_rows.astype(jnp.float32).reshape(token_count, TOP, D), axis=1))
    g_dn = gain32 * d_normed
    inner = lax.optimization_barrier(jnp.mean(mid32 * g_dn, axis=1))
    mid_total = layer_cot.astype(jnp.float32) + inv_rms[:, None] * g_dn - mid32 * (inv_rms ** 3 * inner)[:, None]
    mid_grad = mid_total.astype(jnp.bfloat16)
    b32 = b_gate.astype(jnp.float32)
    y32 = conv_out.astype(jnp.float32)
    grouped = (b32 * y32).reshape(token_count, CONV_CH // GROUP, GROUP)
    group_rms = lax.rsqrt(lax.optimization_barrier(jnp.mean(grouped * grouped, axis=-1)) + epsilon)
    cgain = conv_gain.astype(jnp.float32).reshape(CONV_CH // GROUP, GROUP)
    conv_normed = (grouped * group_rms[..., None] * cgain).reshape(token_count, CONV_CH).astype(jnp.bfloat16)
    grad_out_weight = jnp.dot(mid_grad.T, conv_normed, preferred_element_type=jnp.float32)
    d_normed_conv = jnp.dot(mid_grad, out_weight, preferred_element_type=jnp.float32).reshape(grouped.shape)
    g_dc = cgain * d_normed_conv
    group_inner = lax.optimization_barrier(jnp.mean(grouped * g_dc, axis=-1))
    d_gated = (group_rms[..., None] * g_dc - grouped * (group_rms ** 3 * group_inner)[..., None]).reshape(token_count, CONV_CH)
    grad_b = (d_gated * y32).astype(jnp.bfloat16)
    d_conv_out = d_gated * b32
    extended = jnp.concatenate([d_conv_out, jnp.zeros((2, CONV_CH), jnp.float32)], axis=0)
    taps = conv_taps.astype(jnp.float32)
    d_mixed = taps[2] * extended[:-2] + taps[1] * extended[1:-1] + taps[0] * extended[2:]
    grad_c = (d_mixed * conv_in.astype(jnp.float32)).astype(jnp.bfloat16)
    grad_conv_in = (d_mixed * c_gate.astype(jnp.float32)).astype(jnp.bfloat16)
    return (grad_gate, grad_up, grad_down, grad_out_weight, mid_grad, grad_b, grad_c, grad_conv_in)
```

```python
import functools

import jax
import jax.numpy as jnp
from jax import lax
from jax.experimental import pallas as pl
from jax.experimental.pallas import tpu as pltpu
from jax.sharding import PartitionSpec as P

GROUP = 64
MESH = pl.DeviceIdType.MESH
VMEM_LIMIT = 63 * 1024 * 1024
COL = 256

epsilon = 1e-06

f32, bf16 = jnp.float32, jnp.bfloat16


def from_behind(block, axis, distance):
    devices = range(lax.axis_size(axis))
    route = [(i - distance, i) for i in devices if i - distance in devices]
    return lax.ppermute(block, axis, route)


def silu_parts(pre):
    sigma = jax.nn.sigmoid(pre)
    return (pre * sigma, sigma * (1.0 + pre * (1.0 - sigma)))


def contract_rows(left, right):
    return lax.dot_general(
        left, right, (((0,), (0,)), ((), ())), preferred_element_type=jnp.float32
    )


def contract_cols(left, right):
    return lax.dot_general(
        left, right, (((1,), (1,)), ((), ())), preferred_element_type=jnp.float32
    )


def remote(src, dst, send, recv, where):
    return pltpu.make_async_remote_copy(
        src_ref=src,
        dst_ref=dst,
        send_sem=send,
        recv_sem=recv,
        device_id=where,
        device_id_type=MESH,
    )


def cols_at(start, size):
    return pl.ds(pl.multiple_of(start, size), size)


def greet(planes, plane, z, q, c):
    barrier = pltpu.get_barrier_semaphore()
    me = z * plane + q

    def hello(peer, core):
        pl.semaphore_signal(barrier, inc=1, device_id=(peer, core), device_id_type=MESH)

    @pl.loop(1, plane)
    def _(k):
        hello(z * plane + lax.rem(q + k, plane), c)

    hello(me, 1 - c)

    @pl.when(z > 0)
    def _():
        hello(me - plane, c)

    @pl.when(z < planes - 1)
    def _():
        hello(me + plane, c)

    pl.semaphore_wait(barrier, plane + jnp.minimum(z, 1) + jnp.minimum(planes - 1 - z, 1))


def expert_kernel(
    dims,
    mid_in, cot_in, meta_in, gain, gate_in, up_in, down_in,
    mid_grad, full, tokens_out, cots_out, hid_out, dgate_out, dup_out,
    mid_all, cot_all, meta_all, place, share_col, rows_tok, rows_cot, tokens, cots,
    hid, dgate, dup, active, slope, part, theirs, total, back, chain, dn, inner,
    gate, up, down,
    ld, meta_sem, z_up, z_dn, z_recv, p_send, p_recv, f_send, f_recv, own_sem,
    x_send, x_recv, b_send, b_recv, c_send, c_recv, fin, out_sem,
):
    A, B, cap, R, H, F = dims
    S, W = B * cap, 2 * H
    tiles = H // COL
    me, c = lax.axis_index("sp"), lax.axis_index("tp")
    z, q = lax.div(me, B), lax.rem(me, B)
    partner = (me, 1 - c)
    cols = cols_at(c * H, H)
    other = cols_at((1 - c) * H, H)

    def slots_of(source):
        return cols_at(source * cap, cap)

    def group_of(b):
        return cols_at(b * S, S)

    def order(s):
        low = jnp.minimum(z, A - 1 - z)
        step = lax.div(s + 1, 2)
        near = jnp.where(lax.rem(s, 2) == 1, z - step, z + step)
        far = jnp.where(z < A - 1 - z, s, A - 1 - s)
        return jnp.where(s <= 2 * low, near, far)

    down_first = A - 1 - z <= z

    def chain_order(j):
        below = jnp.where(down_first, z - 1 - j, z - 1 - (j - (A - 1 - z)))
        above = jnp.where(down_first, z + 1 + (j - z), z + 1 + j)
        take_below = jnp.where(down_first, j < z, j >= A - 1 - z)
        return jnp.where(take_below, below, above)

    loads = [
        pltpu.make_async_copy(meta_in, meta_all.at[z, c], ld.at[0]),
        pltpu.make_async_copy(mid_in, mid_all.at[z], ld.at[1]),
        pltpu.make_async_copy(cot_in, cot_all.at[z], ld.at[2]),
        pltpu.make_async_copy(gate_in, gate, ld.at[3]),
        pltpu.make_async_copy(up_in, up, ld.at[4]),
        pltpu.make_async_copy(down_in, down, ld.at[5]),
    ]
    for load in loads:
        load.start()

    greet(A, B, z, q, c)

    remote(meta_in, meta_all.at[z, c], meta_sem.at[0], meta_sem.at[1], partner).start()

    stores = (meta_all, mid_all, cot_all)

    def z_copy(a, b, up_way):
        where = (me + B, c) if up_way else (me - B, c)
        sems = z_up if up_way else z_dn
        return remote(stores[a].at[b], stores[a].at[b], sems.at[a, b], z_recv.at[a, b], where)

    def z_both(a):
        @pl.when(z < A - 1)
        def _():
            z_copy(a, z, True).start()

        @pl.when(z > 0)
        def _():
            z_copy(a, z, False).start()

    loads[0].wait()
    remote(meta_in, meta_all.at[z, 1 - c], meta_sem.at[0], meta_sem.at[1], partner).wait()
    z_both(0)
    loads[1].wait()
    z_both(1)
    loads[2].wait()
    z_both(2)

    def arrive(a, b):
        @pl.when(b != z)
        def _():
            remote(
                stores[a].at[b], stores[a].at[b], z_up.at[a, b], z_recv.at[a, b], partner
            ).wait_recv()

            @pl.when((b < z) & (z < A - 1))
            def _():
                z_copy(a, b, True).start()

            @pl.when((b > z) & (z > 0))
            def _():
                z_copy(a, b, False).start()

    rows = (rows_tok, rows_cot)
    inbox = (tokens, cots)

    def plane_send(a, b, k):
        peer = lax.rem(q + k, B)
        return remote(
            rows[a].at[slots_of(peer)],
            inbox[a].at[slots_of(b * B + q), cols],
            p_send.at[a, k],
            p_recv.at[a, b, k],
            (z * B + peer, c),
        )

    def plane_incoming(a, b, k):
        source = lax.rem(q + B - k, B)
        spot = inbox[a].at[slots_of(b * B + source), cols]
        return remote(spot, spot, p_send.at[a, k], p_recv.at[a, b, k], partner)

    def forward(a, b, k):
        source = lax.rem(q + B - k, B)
        spot = inbox[a].at[slots_of(b * B + source), cols]
        return remote(spot, spot, f_send.at[a, b, k], f_recv.at[a, b, k], partner)

    def forwarded(a, b, k):
        source = lax.rem(q + B - k, B)
        spot = inbox[a].at[slots_of(b * B + source), other]
        return remote(spot, spot, f_send.at[a, b, k], f_recv.at[a, b, k], partner)

    def own_local(a, b):
        return pltpu.make_async_copy(
            rows[a].at[slots_of(q)], inbox[a].at[slots_of(b * B + q), cols], own_sem.at[a]
        )

    def own_partner(a, b):
        return remote(
            rows[a].at[slots_of(q)],
            inbox[a].at[slots_of(b * B + q), cols],
            f_send.at[a, b, 0],
            f_recv.at[a, b, 0],
            partner,
        )

    def rows_out(a, b):
        @pl.loop(1, B)
        def _(k):
            plane_send(a, b, k).start()

        own_local(a, b).start()
        own_partner(a, b).start()

    def rows_sent(a, b):
        @pl.loop(1, B)
        def _(k):
            plane_send(a, b, k).wait_send()

        own_local(a, b).wait()
        own_partner(a, b).wait_send()

    def meta_rows(b):
        first, second = meta_all[b, 0], meta_all[b, 1]
        inv = lax.rsqrt((first[4:5] + second[4:5]) / W + epsilon)
        base = lax.convert_element_type(z * S, f32)
        return first[0:1] - base, first[1:2] - base, first[2:3], first[3:4], inv

    def pick_tokens(b):
        slot0, slot1, share0, share1, inv = meta_rows(b)
        slot = lax.broadcasted_iota(jnp.int32, (S, R), 0).astype(f32)
        at0, at1 = slot == slot0, slot == slot1
        hit = at0 | at1
        place[b] = jnp.where(hit, 1.0, 0.0).astype(bf16)
        inv_col = jnp.sum(jnp.where(hit, inv, 0.0), axis=1, keepdims=True)
        share_col[...] = jnp.sum(
            jnp.where(at0, share0, jnp.where(at1, share1, 0.0)), axis=1, keepdims=True
        )

        @pl.loop(0, tiles)
        def _(t):
            tile = cols_at(t * COL, COL)
            picked = jnp.dot(place[b], mid_all[b, :, tile], preferred_element_type=f32)
            rows_tok[:, tile] = (picked * inv_col * gain[:, tile]).astype(bf16)

        rows_out(0, b)

    def pick_cots(b):
        @pl.loop(0, tiles)
        def _(t):
            tile = cols_at(t * COL, COL)
            picked = jnp.dot(place[b], cot_all[b, :, tile], preferred_element_type=f32)
            rows_cot[:, tile] = (picked * share_col[...]).astype(bf16)

        rows_out(1, b)

    def swap(b):
        return remote(
            part.at[:, other], theirs.at[b], x_send.at[b], x_recv.at[b], partner
        )

    def give_back(b, k):
        peer = lax.rem(q + k, B)
        return remote(
            total.at[slots_of(peer)],
            back.at[b, slots_of(q)],
            b_send.at[k],
            b_recv.at[b, k],
            (z * B + peer, c),
        )

    def given_back(b, k):
        spot = back.at[b, slots_of(lax.rem(q + B - k, B))]
        return remote(spot, spot, b_send.at[k], b_recv.at[b, k], partner)

    def outs_of(b):
        pairs = (
            (tokens, tokens_out), (cots, cots_out), (hid, hid_out), (dgate, dgate_out), (dup, dup_out)
        )
        return [
            pltpu.make_async_copy(src.at[group_of(b)], dst.at[group_of(b)], out_sem.at[a, b])
            for a, (src, dst) in enumerate(pairs)
        ]

    def run_experts(i):
        b = order(i)
        here = group_of(b)

        for a in range(2):
            @pl.loop(1, B)
            def _(k):
                plane_incoming(a, b, k).wait_recv()
                forward(a, b, k).start()

        @pl.loop(0, B)
        def _(k):
            forwarded(0, b, k).wait_recv()

        @pl.loop(0, F // COL)
        def _(t):
            tile = cols_at(t * COL, COL)
            pre_gate = jnp.dot(tokens[here, :], gate[:, tile], preferred_element_type=f32)
            pre_up = jnp.dot(tokens[here, :], up[:, tile], preferred_element_type=f32)
            lit, lean = silu_parts(pre_gate)
            hid[here, tile] = (lit * pre_up).astype(bf16)
            active[:, tile] = lit
            slope[:, tile] = pre_up * lean

        @pl.loop(0, B)
        def _(k):
            forwarded(1, b, k).wait_recv()

        @pl.loop(0, F // COL)
        def _(t):
            tile = cols_at(t * COL, COL)
            d_hidden = contract_cols(cots[here, :], down[tile, :])
            dgate[here, tile] = (d_hidden * slope[:, tile]).astype(bf16)
            dup[here, tile] = (d_hidden * active[:, tile]).astype(bf16)

        for copy in outs_of(b):
            copy.start()

        @pl.when(i > 0)
        def _():
            swap(order(i - 1)).wait_send()

        def part_half(core):
            @pl.loop(0, tiles)
            def _(t):
                tile = cols_at(core * H + t * COL, COL)
                got = contract_cols(dgate[here, :], gate[tile, :])
                got = got + contract_cols(dup[here, :], up[tile, :])
                part[:, tile] = got.astype(bf16)

        part_half(1 - c)
        swap(b).start()
        part_half(c)

        @pl.when(i > 0)
        def _():
            @pl.loop(1, B)
            def _(k):
                give_back(order(i - 1), k).wait_send()

        swap(b).wait_recv()

        @pl.loop(1, B + 1)
        def _(k):
            peer = lax.rem(q + k, B)
            total[slots_of(peer), :] = (
                part[slots_of(peer), cols].astype(f32) + theirs[b, slots_of(peer), :].astype(f32)
            ).astype(bf16)

        @pl.loop(1, B)
        def _(k):
            give_back(b, k).start()

        back[b, slots_of(q), :] = total[slots_of(q), :]

    def all_back(b):
        @pl.loop(1, B)
        def _(k):
            given_back(b, k).wait_recv()

    def chain_copy(b, t, up_way):
        tile = cols_at(t * COL, COL)
        if up_way:
            spot = jnp.where(b == z + 1, A, b)
            where = (me + B, c)
        else:
            spot, where = b, (me - B, c)
        return remote(
            chain.at[b, :, tile], chain.at[spot, :, tile], c_send.at[b, t], c_recv.at[spot, t], where
        )

    def chain_arrives(spot, t):
        at = chain.at[spot, :, cols_at(t * COL, COL)]
        remote(at, at, c_send.at[spot, t], c_recv.at[spot, t], partner).wait_recv()

    def pass_on(j):
        b = chain_order(j)
        all_back(b)
        fed = ((b < z) & (z < A - 1)) | ((b > z) & (z > 0))

        @pl.loop(0, tiles)
        def _(t):
            tile = cols_at(t * COL, COL)
            mine = contract_rows(place[b], back[b, :, tile])

            @pl.when(fed)
            def _():
                chain_arrives(b, t)
                chain[b, :, tile] = (mine + chain[b, :, tile].astype(f32)).astype(bf16)

            @pl.when(jnp.logical_not(fed))
            def _():
                chain[b, :, tile] = mine.astype(bf16)

            @pl.when(b < z)
            def _():
                chain_copy(b, t, False).start()

            @pl.when(b > z)
            def _():
                chain_copy(b, t, True).start()

    at_end = (z == 0) | (z == A - 1)

    @pl.loop(0, A)
    def _(i):
        b = order(i)
        arrive(0, b)
        arrive(1, b)

        @pl.when(i > 0)
        def _():
            rows_sent(0, order(i - 1))
            rows_sent(1, order(i - 1))

        pick_tokens(b)

        @pl.when(i == 0)
        def _():
            for load in loads[3:]:
                load.wait()

        @pl.when(i > 0)
        def _():
            run_experts(i - 1)

        arrive(2, b)
        pick_cots(b)

        @pl.when(at_end & (i > 1))
        def _():
            pass_on(i - 2)

    rows_sent(0, order(A - 1))
    rows_sent(1, order(A - 1))
    run_experts(A - 1)

    @pl.loop(0, A - 1)
    def _(j):
        @pl.when(jnp.logical_not(at_end) | (j == A - 2))
        def _():
            pass_on(j)

    all_back(z)
    inner[0] = jnp.zeros((R, 128), f32)

    @pl.loop(0, tiles)
    def _(t):
        tile = cols_at(t * COL, COL)
        dn[:, tile] = contract_rows(place[z], back[z, :, tile])

        @pl.when(z < A - 1)
        def _():
            chain_arrives(z, t)
            dn[:, tile] += chain[z, :, tile].astype(f32)

        @pl.when(z > 0)
        def _():
            chain_arrives(A, t)
            dn[:, tile] += chain[A, :, tile].astype(f32)

        g_dn = gain[:, tile] * dn[:, tile]
        dn[:, tile] = g_dn
        summed = jnp.sum(mid_all[z, :, tile].astype(f32) * g_dn, axis=1, keepdims=True)
        inner[0] += jnp.broadcast_to(summed, (R, 128))

    share_inner = remote(inner.at[0], inner.at[1], fin.at[0], fin.at[1], partner)
    share_inner.start()
    inv = meta_rows(z)[4]
    eye = lax.broadcasted_iota(jnp.int32, (R, R), 0) == lax.broadcasted_iota(jnp.int32, (R, R), 1)
    inv_tok = jnp.sum(jnp.where(eye, inv, 0.0), axis=1, keepdims=True)
    share_inner.wait()
    drop = inv_tok * inv_tok * inv_tok * ((inner[0, :, 0:1] + inner[1, :, 0:1]) / W)

    @pl.loop(0, tiles)
    def _(t):
        tile = cols_at(t * COL, COL)
        turned = (
            cot_all[z, :, tile].astype(f32)
            + inv_tok * dn[:, tile]
            - mid_all[z, :, tile].astype(f32) * drop
        ).astype(bf16)
        mid_grad[:, tile] = turned
        full[:, cols_at(c * H + t * COL, COL)] = turned

    share_mid = remote(full.at[:, cols], full.at[:, cols], fin.at[2], fin.at[3], partner)
    share_mid.start()

    @pl.loop(0, A)
    def _(b):
        for copy in outs_of(b):
            copy.wait()
        for a in range(2):
            @pl.loop(1, B)
            def _(k):
                forward(a, b, k).wait_send()

        for a in range(3):
            @pl.when((b <= z) & (z < A - 1))
            def _():
                z_copy(a, b, True).wait_send()

            @pl.when((b >= z) & (z > 0))
            def _():
                z_copy(a, b, False).wait_send()

        @pl.loop(0, tiles)
        def _(t):
            @pl.when(b < z)
            def _():
                chain_copy(b, t, False).wait_send()

            @pl.when(b > z)
            def _():
                chain_copy(b, t, True).wait_send()

    swap(order(A - 1)).wait_send()

    @pl.loop(1, B)
    def _(k):
        give_back(order(A - 1), k).wait_send()

    share_mid.wait_send()
    remote(full.at[:, other], full.at[:, other], fin.at[2], fin.at[3], partner).wait_recv()


def experts(mid, cot, meta, gain, gate, up, down, n, cap, plane, ident):
    R, H = mid.shape
    F = gate.shape[1]
    W = 2 * H
    B = plane
    A = n // B
    S = B * cap
    anywhere = pl.BlockSpec(memory_space=pl.ANY)
    vmem = pl.BlockSpec(memory_space=pltpu.VMEM)
    dma = pltpu.SemaphoreType.DMA
    tiles = H // COL
    dims = (A, B, cap, R, H, F)
    return pl.pallas_call(
        functools.partial(expert_kernel, dims),
        out_shape=(
            jax.ShapeDtypeStruct((R, H), bf16),
            jax.ShapeDtypeStruct((R, W), bf16),
            jax.ShapeDtypeStruct((A * S, W), bf16),
            jax.ShapeDtypeStruct((A * S, W), bf16),
            jax.ShapeDtypeStruct((A * S, F), bf16),
            jax.ShapeDtypeStruct((A * S, F), bf16),
            jax.ShapeDtypeStruct((A * S, F), bf16),
        ),
        in_specs=[anywhere, anywhere, vmem, vmem, anywhere, anywhere, anywhere],
        out_specs=(vmem, vmem) + (anywhere,) * 5,
        scratch_shapes=[
            pltpu.VMEM((A, R, H), bf16),
            pltpu.VMEM((A, R, H), bf16),
            pltpu.VMEM((A, 2, 8, R), f32),
            pltpu.VMEM((A, S, R), bf16),
            pltpu.VMEM((S, 1), f32),
            pltpu.VMEM((S, H), bf16),
            pltpu.VMEM((S, H), bf16),
            pltpu.VMEM((A * S, W), bf16),
            pltpu.VMEM((A * S, W), bf16),
            pltpu.VMEM((A * S, F), bf16),
            pltpu.VMEM((A * S, F), bf16),
            pltpu.VMEM((A * S, F), bf16),
            pltpu.VMEM((S, F), f32),
            pltpu.VMEM((S, F), f32),
            pltpu.VMEM((S, W), bf16),
            pltpu.VMEM((A, S, H), bf16),
            pltpu.VMEM((S, H), bf16),
            pltpu.VMEM((A, S, H), bf16),
            pltpu.VMEM((A + 1, R, H), bf16),
            pltpu.VMEM((R, H), f32),
            pltpu.VMEM((2, R, 128), f32),
            pltpu.VMEM((W, F), bf16),
            pltpu.VMEM((W, F), bf16),
            pltpu.VMEM((F, W), bf16),
            dma((6,)),
            dma((2,)),
            dma((3, A)),
            dma((3, A)),
            dma((3, A)),
            dma((2, B)),
            dma((2, A, B)),
            dma((2, A, B)),
            dma((2, A, B)),
            dma((2,)),
            dma((A,)),
            dma((A,)),
            dma((B,)),
            dma((A, B)),
            dma((A, tiles)),
            dma((A + 1, tiles)),
            dma((4,)),
            dma((5, A)),
        ],
        compiler_params=pltpu.CompilerParams(
            collective_id=ident, has_side_effects=True, vmem_limit_bytes=VMEM_LIMIT
        ),
        name="experts",
    )(mid, cot, meta, gain, gate, up, down)


def combine_kernel(dims, full, normed, out, term, plane_in, line_out, line_in, p_send, p_recv, l_send, l_recv):
    A, B, rows, F = dims
    me, c = lax.axis_index("sp"), lax.axis_index("tp")
    z, q = lax.div(me, B), lax.rem(me, B)
    barrier = pltpu.get_barrier_semaphore()

    @pl.loop(1, B)
    def _(k):
        pl.semaphore_signal(
            barrier, inc=1, device_id=(z * B + lax.rem(q + k, B), c), device_id_type=MESH
        )

    @pl.loop(1, A)
    def _(j):
        pl.semaphore_signal(
            barrier, inc=1, device_id=(lax.rem(z + j, A) * B + q, c), device_id_type=MESH
        )

    def lot(x):
        return pl.ds(pl.multiple_of(x * rows, rows), rows)

    def plane_send(s, k):
        peer = lax.rem(q + k, B)
        return remote(
            term.at[s, lot(peer)], plane_in.at[s, k], p_send.at[s, k], p_recv.at[s, k],
            (z * B + peer, c),
        )

    def line_send(s):
        return remote(
            line_out.at[s], line_in.at[s], l_send.at[s], l_recv.at[s],
            (lax.rem(z + s, A) * B + q, c),
        )

    def product(s):
        block = cols_at(lax.rem(z + s, A) * (B * rows), B * rows)
        got = contract_rows(full[:, block], normed[...])
        term[s] = got.astype(bf16)

    @pl.loop(0, A)
    def _(j):
        s = A - 1 - j
        product(s)

        @pl.when(j == 0)
        def _():
            pl.semaphore_wait(barrier, A + B - 2)

        @pl.loop(1, B)
        def _(k):
            plane_send(s, k).start()

    def plane_sum(s):
        out[...] = term[s, lot(q), :].astype(f32)

        @pl.loop(1, B)
        def _(k):
            plane_send(s, k).wait_recv()
            out[...] += plane_in[s, k].astype(f32)

    @pl.loop(0, A - 1)
    def _(j):
        s = A - 1 - j
        plane_sum(s)
        line_out[s] = out[...].astype(bf16)
        line_send(s).start()

    plane_sum(0)

    @pl.loop(1, A)
    def _(s):
        line_send(s).wait_recv()
        out[...] += line_in[s].astype(f32)

    @pl.loop(0, A)
    def _(s):
        @pl.loop(1, B)
        def _(k):
            plane_send(s, k).wait_send()

        @pl.when(s > 0)
        def _():
            line_send(s).wait_send()


def combine(full, normed, n, plane, ident):
    R, W = full.shape
    F = normed.shape[1]
    A, B = n // plane, plane
    rows = W // n
    vmem = pl.BlockSpec(memory_space=pltpu.VMEM)
    dma = pltpu.SemaphoreType.DMA
    return pl.pallas_call(
        functools.partial(combine_kernel, (A, B, rows, F)),
        out_shape=jax.ShapeDtypeStruct((rows, F), f32),
        in_specs=[vmem, vmem],
        out_specs=vmem,
        scratch_shapes=[
            pltpu.VMEM((A, B * rows, F), bf16),
            pltpu.VMEM((A, B, rows, F), bf16),
            pltpu.VMEM((A, rows, F), bf16),
            pltpu.VMEM((A, rows, F), bf16),
            dma((A, B)),
            dma((A, B)),
            dma((A,)),
            dma((A,)),
        ],
        compiler_params=pltpu.CompilerParams(
            collective_id=ident, has_side_effects=True, vmem_limit_bytes=VMEM_LIMIT
        ),
        name="combine",
    )(full, normed)


def group_mean(values, blocks):
    return jnp.dot(
        values, blocks, precision=lax.Precision.HIGHEST, preferred_element_type=jnp.float32
    ) * (1.0 / GROUP)


def shards(
    mid_stream,
    layer_cot,
    ffn_gain,
    expert_ids,
    group_prob,
    first_share,
    expert_gate,
    expert_up,
    expert_down,
    out_weight,
    conv_gain,
    b_gate,
    c_gate,
    conv_in,
    conv_out,
    conv_taps,
):
    row_count, half_width = mid_stream.shape
    n = lax.axis_size("sp")
    expert_count = n * expert_gate.shape[0]
    slot_count = 4 * row_count // expert_count
    plane = row_count // slot_count
    cap = -(-slot_count // 16) * 16

    mid32 = mid_stream.astype(f32)
    square_sum = jnp.sum(mid32 * mid32, axis=1)
    experts_row = jnp.arange(expert_count, dtype=jnp.int32)[None, :]
    hot = [expert_ids[:, c : c + 1] == experts_row for c in range(2)]
    both = jnp.concatenate([h.astype(bf16) for h in hot], axis=1)
    row = jnp.arange(row_count, dtype=jnp.int32)
    before = (row[None, :] < row[:, None]).astype(bf16)
    counted = jnp.dot(before, both, preferred_element_type=f32)
    first_total = jnp.sum(hot[0].astype(f32), axis=0, keepdims=True)
    rank0 = jnp.sum(jnp.where(hot[0], counted[:, :expert_count], 0.0), axis=1)
    rank1 = jnp.sum(jnp.where(hot[1], counted[:, expert_count:] + first_total, 0.0), axis=1)
    ids = expert_ids.astype(f32)
    none = jnp.zeros_like(rank0)
    meta = jnp.stack(
        [
            ids[:, 0] * cap + rank0,
            ids[:, 1] * cap + rank1,
            group_prob * first_share,
            group_prob * (1.0 - first_share),
            square_sum,
            none,
            none,
            none,
        ],
        axis=0,
    )
    gain32 = ffn_gain.astype(f32)[None, :]
    gate_w, up_w, down_w = expert_gate[0], expert_up[0], expert_down[0]
    mid_grad, full_mid, tokens_in, cots_in, hidden, d_gate, d_up = experts(
        mid_stream, layer_cot, meta, gain32, gate_w, up_w, down_w, n, cap, plane, 1
    )

    channel_count = b_gate.shape[1]
    b32 = b_gate.astype(f32)
    y32 = conv_out.astype(f32)
    gated = b32 * y32
    lane = jnp.arange(channel_count, dtype=jnp.int32) // GROUP
    blocks = (lane[:, None] == lane[None, :]).astype(f32)
    group_rms = lax.rsqrt(group_mean(gated * gated, blocks) + epsilon)
    cgain = conv_gain.astype(f32)[None, :]
    conv_normed = (gated * group_rms * cgain).astype(bf16)

    grad_out_weight = combine(full_mid, conv_normed, n, plane, 2)

    d_normed_conv = jnp.dot(full_mid, out_weight, preferred_element_type=f32)
    g_dc = cgain * d_normed_conv
    group_inner = group_mean(gated * g_dc, blocks)
    d_gated = group_rms * g_dc - gated * (group_rms**3 * group_inner)
    grad_b = (d_gated * y32).astype(bf16)
    d_conv_out = d_gated * b32
    following = from_behind(d_conv_out[:2], "sp", -1)
    grad_down = contract_rows(hidden, cots_in)[None]
    grad_gate = contract_rows(tokens_in, d_gate)[None]
    grad_up = contract_rows(tokens_in, d_up)[None]
    extended = jnp.concatenate([d_conv_out, following], axis=0)
    taps = conv_taps.astype(f32)
    d_mixed = taps[2] * extended[:-2] + taps[1] * extended[1:-1] + taps[0] * extended[2:]
    grad_c = (d_mixed * conv_in.astype(f32)).astype(bf16)
    grad_conv_in = (d_mixed * c_gate.astype(f32)).astype(bf16)
    return (grad_gate, grad_up, grad_down, grad_out_weight, mid_grad, grad_b, grad_c, grad_conv_in)


def solution(mesh):
    placed = (
        P("sp", "tp"),
        P("sp", "tp"),
        P("tp"),
        P("sp", None),
        P("sp"),
        P("sp"),
        P("sp", None, "tp"),
        P("sp", None, "tp"),
        P("sp", "tp", None),
        P(None, "tp"),
        P("tp"),
        P("sp", "tp"),
        P("sp", "tp"),
        P("sp", "tp"),
        P("sp", "tp"),
        P(None, "tp"),
    )
    return jax.shard_map(
        shards,
        mesh=mesh,
        in_specs=placed,
        out_specs=(
            P("sp", None, "tp"),
            P("sp", None, "tp"),
            P("sp", "tp", None),
            P("sp", "tp"),
            P("sp", "tp"),
            P("sp", "tp"),
            P("sp", "tp"),
            P("sp", "tp"),
        ),
        check_vma=False,
    )
```

```python
import functools

import jax
import jax.numpy as jnp
from jax import lax
from jax.experimental import pallas as pl
from jax.experimental.pallas import tpu as pltpu
from jax.sharding import PartitionSpec as P

GROUP = 64
MESH = pl.DeviceIdType.MESH
VMEM_LIMIT = 63 * 1024 * 1024
COL = 256
HALVES = 2

epsilon = 1e-06

f32, bf16 = jnp.float32, jnp.bfloat16


def from_behind(block, axis, distance):
    devices = range(lax.axis_size(axis))
    route = [(i - distance, i) for i in devices if i - distance in devices]
    return lax.ppermute(block, axis, route)


def silu_parts(pre):
    sigma = jax.nn.sigmoid(pre)
    return (pre * sigma, sigma * (1.0 + pre * (1.0 - sigma)))


def contract_rows(left, right):
    return lax.dot_general(
        left, right, (((0,), (0,)), ((), ())), preferred_element_type=jnp.float32
    )


def contract_cols(left, right):
    return lax.dot_general(
        left, right, (((1,), (1,)), ((), ())), preferred_element_type=jnp.float32
    )


def remote(src, dst, send, recv, where):
    return pltpu.make_async_remote_copy(
        src_ref=src,
        dst_ref=dst,
        send_sem=send,
        recv_sem=recv,
        device_id=where,
        device_id_type=MESH,
    )


def cols_at(start, size):
    return pl.ds(pl.multiple_of(start, size), size)


def greet(planes, plane, z, q, c):
    barrier = pltpu.get_barrier_semaphore()
    me = z * plane + q

    def hello(peer, core):
        pl.semaphore_signal(barrier, inc=1, device_id=(peer, core), device_id_type=MESH)

    @pl.loop(1, plane)
    def _(k):
        hello(z * plane + lax.rem(q + k, plane), c)

    hello(me, 1 - c)

    @pl.when(z > 0)
    def _():
        hello(me - plane, c)

    @pl.when(z < planes - 1)
    def _():
        hello(me + plane, c)

    pl.semaphore_wait(barrier, plane + jnp.minimum(z, 1) + jnp.minimum(planes - 1 - z, 1))


def expert_kernel(
    dims,
    mid_in, cot_in, ids, group_prob, first_share, gain_in, gate_in, up_in, down_in,
    mid_grad, full, tokens_out, cots_out, hid_out, dgate_out, dup_out,
    mid_all, cot_all, meta_all, place, inv_col, share_col, rows_tok, rows_cot, tokens, cots,
    hid, dgate, dup, active, slope, part, theirs, total, back, chain, dn, inner, gain,
    gate, up, down,
    ld, meta_sem, z_up, z_dn, z_recv, p_send, p_recv, f_send, f_recv, own_sem,
    x_send, x_recv, b_send, b_recv, c_send, c_recv, fin, out_sem,
):
    A, B, cap, R, H, F = dims
    S, W = B * cap, 2 * H
    tiles = H // COL
    me, c = lax.axis_index("sp"), lax.axis_index("tp")
    z, q = lax.div(me, B), lax.rem(me, B)
    partner = (me, 1 - c)
    cols = cols_at(c * H, H)
    other = cols_at((1 - c) * H, H)

    def slots_of(source):
        return cols_at(source * cap, cap)

    def group_of(b):
        return cols_at(b * S, S)

    above_count = A - 1 - z

    def from_below(r):
        tok = r <= z
        return (r >= 1) & (r <= 2 * z), tok, jnp.where(tok, z - r, r - z - 1)

    def from_above(r):
        tok = r <= above_count
        valid = (r >= 1) & (r <= 2 * above_count)
        return valid, tok, jnp.where(tok, z + r, A + above_count - r)

    sides = (from_below, from_above)

    loads = [
        pltpu.make_async_copy(mid_in, mid_all.at[z], ld.at[0]),
        pltpu.make_async_copy(cot_in, cot_all.at[z], ld.at[1]),
        pltpu.make_async_copy(gate_in, gate, ld.at[2]),
        pltpu.make_async_copy(up_in, up, ld.at[3]),
        pltpu.make_async_copy(down_in, down, ld.at[4]),
    ]
    for load in loads:
        load.start()

    greet(A, B, z, q, c)

    def note_slots():
        crowd = A * B
        row = lax.broadcasted_iota(jnp.int32, (R, R), 0)
        col = lax.broadcasted_iota(jnp.int32, (R, R), 1)
        before = jnp.where(row < col, 1.0, 0.0).astype(bf16)
        expert = lax.broadcasted_iota(jnp.int32, (crowd, R), 0)
        hot = [jnp.where(ids[k : k + 1, :] == expert, 1.0, 0.0) for k in range(2)]
        counted = [jnp.dot(h.astype(bf16), before, preferred_element_type=f32) for h in hot]
        counted[1] = counted[1] + jnp.sum(hot[0], axis=1, keepdims=True)
        squares = jnp.zeros((R, 1), f32)
        for t in range(tiles):
            own = mid_all[z, :, t * COL : (t + 1) * COL].astype(f32)
            squares = squares + jnp.sum(own * own, axis=1, keepdims=True)

        for k in range(2):
            rank = jnp.sum(hot[k] * counted[k], axis=0, keepdims=True)
            meta_all[z, c, k : k + 1, :] = ids[k : k + 1, :].astype(f32) * cap + rank
        prob, first = group_prob[...].reshape(1, R), first_share[...].reshape(1, R)
        meta_all[z, c, 2:3, :] = prob * first
        meta_all[z, c, 3:4, :] = prob * (1.0 - first)
        meta_all[z, c, 4:5, :] = jnp.sum(jnp.where(row == col, squares, 0.0), axis=0, keepdims=True)
        meta_all[z, c, 5:8, :] = jnp.zeros((3, R), f32)
        gain[...] = gain_in[...].astype(f32).reshape(1, H)
        mine = meta_all.at[z, c]
        remote(mine, mine, meta_sem.at[0], meta_sem.at[1], partner).start()
        theirs_at = meta_all.at[z, 1 - c]
        remote(theirs_at, theirs_at, meta_sem.at[0], meta_sem.at[1], partner).wait()

    wide = H // HALVES
    stores = (mid_all, cot_all)

    def piece(h):
        return cols_at(h * wide, wide)

    def z_spot(a, h, b):
        return meta_all.at[b] if a == 2 else stores[a].at[b, :, piece(h)]

    def z_copy(a, h, b, up_way):
        where = (me + B, c) if up_way else (me - B, c)
        sems = z_up if up_way else z_dn
        spot = z_spot(a, h, b)
        return remote(spot, spot, sems.at[a, b], z_recv.at[a, h, b], where)

    def z_own(a, h):
        @pl.when(z < A - 1)
        def _():
            z_copy(a, h, z, True).start()

        @pl.when(z > 0)
        def _():
            z_copy(a, h, z, False).start()

    loads[0].wait()
    for h in range(HALVES):
        z_own(0, h)
    note_slots()
    z_own(2, 0)
    loads[1].wait()

    @pl.when(z == 0)
    def _():
        for h in range(HALVES):
            z_copy(1, h, z, True).start()

    @pl.when(z == A - 1)
    def _():
        for h in range(HALVES):
            z_copy(1, h, z, False).start()

    def landed(a, h, b):
        at = z_spot(a, h, b)
        remote(at, at, z_up.at[a, b], z_recv.at[a, h, b], partner).wait_recv()

    def arrive(r, h):
        for up_way, side in ((True, from_below), (False, from_above)):
            valid, tok, b = side(r)
            onward = (z < A - 1) if up_way else (z > 0)
            last = r == (2 * z if up_way else 2 * above_count)

            @pl.when(valid & tok)
            def _():
                landed(0, h, b)

                @pl.when(onward)
                def _():
                    z_copy(0, h, b, up_way).start()

            @pl.when(valid & tok & (h == HALVES - 1))
            def _():
                landed(2, 0, b)

                @pl.when(onward)
                def _():
                    z_copy(2, 0, b, up_way).start()

            @pl.when(valid & jnp.logical_not(tok))
            def _():
                landed(1, h, b)

                @pl.when(onward)
                def _():
                    z_copy(1, h, b, up_way).start()

            @pl.when(valid & last & onward & (h == HALVES - 1))
            def _():
                for own_h in range(HALVES):
                    z_copy(1, own_h, z, up_way).start()

    rows = (rows_tok, rows_cot)
    inbox = (tokens, cots)

    def in_half(core, h):
        return cols_at(core * H + h * wide, wide)

    def plane_send(a, h, b, k):
        peer = lax.rem(q + k, B)
        return remote(
            rows[a].at[b, slots_of(peer), piece(h)],
            inbox[a].at[slots_of(b * B + q), in_half(c, h)],
            p_send.at[a],
            p_recv.at[a, h, b],
            (z * B + peer, c),
        )

    def plane_landed(a, h, b):
        spot = rows[a].at[b, pl.ds(0, (B - 1) * cap), piece(h)]
        remote(spot, spot, p_send.at[a], p_recv.at[a, h, b], partner).wait_recv()

    def own_local(a, h, b):
        return pltpu.make_async_copy(
            rows[a].at[b, slots_of(q), piece(h)],
            inbox[a].at[slots_of(b * B + q), in_half(c, h)],
            own_sem.at[a, h, b],
        )

    def forward(a, h, b):
        spot = inbox[a].at[group_of(b), in_half(c, h)]
        return remote(spot, spot, f_send.at[a], f_recv.at[a, b], partner)

    def rows_out(a, h, b):
        @pl.loop(1, B)
        def _(k):
            plane_send(a, h, b, k).start()

        own_local(a, h, b).start()

    def meta_rows(b):
        first, second = meta_all[b, 0], meta_all[b, 1]
        inv = lax.rsqrt((first[4:5] + second[4:5]) / W + epsilon)
        base = lax.convert_element_type(z * S, f32)
        return first[0:1] - base, first[1:2] - base, first[2:3], first[3:4], inv

    def find_slots(b):
        slot0, slot1, share0, share1, inv = meta_rows(b)
        slot = lax.broadcasted_iota(jnp.int32, (S, R), 0).astype(f32)
        at0, at1 = slot == slot0, slot == slot1
        hit = at0 | at1
        place[b] = jnp.where(hit, 1.0, 0.0).astype(bf16)
        inv_col[b] = jnp.sum(jnp.where(hit, inv, 0.0), axis=1, keepdims=True)
        share_col[b] = jnp.sum(
            jnp.where(at0, share0, jnp.where(at1, share1, 0.0)), axis=1, keepdims=True
        )

    def pick(a, h, b):
        @pl.loop(0, wide // COL)
        def _(t):
            tile = cols_at(h * wide + t * COL, COL)
            picked = jnp.dot(place[b], stores[a][b, :, tile], preferred_element_type=f32)
            if a == 0:
                rows_tok[b, :, tile] = (picked * inv_col[b] * gain[:, tile]).astype(bf16)
            else:
                rows_cot[b, :, tile] = (picked * share_col[b]).astype(bf16)

        rows_out(a, h, b)

    def swap(b, t):
        tile = cols_at(t * COL, COL)
        return remote(
            part.at[:, cols_at((1 - c) * H + t * COL, COL)],
            theirs.at[b, :, tile],
            x_send.at[t],
            x_recv.at[b, t],
            partner,
        )

    def give_back(b, k, t):
        peer = lax.rem(q + k, B)
        tile = cols_at(t * COL, COL)
        return remote(
            total.at[slots_of(peer), tile],
            back.at[b, slots_of(q), tile],
            b_send.at[t],
            b_recv.at[b, t],
            (z * B + peer, c),
        )

    def given_to(b, t):
        spot = back.at[b, pl.ds(0, (B - 1) * cap), cols_at(t * COL, COL)]
        return remote(spot, spot, b_send.at[t], b_recv.at[b, t], partner)

    def outs_of(b):
        pairs = (
            (tokens, tokens_out), (cots, cots_out), (hid, hid_out), (dgate, dgate_out), (dup, dup_out)
        )
        return [
            pltpu.make_async_copy(src.at[group_of(b)], dst.at[group_of(b)], out_sem.at[a])
            for a, (src, dst) in enumerate(pairs)
        ]

    def take_in(a, b):
        for h in range(HALVES):
            plane_landed(a, h, b)
            own_local(a, h, b).wait()
            forward(a, h, b).start()

    def taken_in(a, b):
        spot = inbox[a].at[group_of(b), other]
        remote(spot, spot, f_send.at[a], f_recv.at[a, b], partner).wait_recv()

    def run_forward(b):
        here = group_of(b)
        taken_in(0, b)

        @pl.loop(0, F // COL)
        def _(t):
            tile = cols_at(t * COL, COL)
            pre_gate = jnp.dot(tokens[here, :], gate[:, tile], preferred_element_type=f32)
            pre_up = jnp.dot(tokens[here, :], up[:, tile], preferred_element_type=f32)
            lit, lean = silu_parts(pre_gate)
            hid[here, tile] = (lit * pre_up).astype(bf16)
            active[here, tile] = lit
            slope[here, tile] = pre_up * lean

    def run_backward(b, before):
        here = group_of(b)
        taken_in(1, b)

        @pl.loop(0, F // COL)
        def _(t):
            tile = cols_at(t * COL, COL)
            d_hidden = contract_cols(cots[here, :], down[tile, :])
            dgate[here, tile] = (d_hidden * slope[here, tile]).astype(bf16)
            dup[here, tile] = (d_hidden * active[here, tile]).astype(bf16)

        for copy in outs_of(b):
            copy.start()

        def part_tile(core, t):
            tile = cols_at(core * H + t * COL, COL)
            got = contract_cols(dgate[here, :], gate[tile, :])
            got = got + contract_cols(dup[here, :], up[tile, :])
            part[:, tile] = got.astype(bf16)

        @pl.loop(0, tiles)
        def _(t):
            @pl.when(before >= 0)
            def _():
                swap(before, t).wait_send()

            part_tile(1 - c, t)
            swap(b, t).start()

        @pl.loop(0, tiles)
        def _(t):
            part_tile(c, t)

            @pl.when(before >= 0)
            def _():
                given_to(b, t).wait_send()

            swap(b, t).wait_recv()
            tile = cols_at(t * COL, COL)
            total[:, tile] = (
                part[:, cols_at(c * H + t * COL, COL)].astype(f32) + theirs[b, :, tile].astype(f32)
            ).astype(bf16)

            @pl.loop(1, B)
            def _(k):
                give_back(b, k, t).start()

            back[b, slots_of(q), tile] = total[slots_of(q), tile]

    def all_back(b, t):
        given_to(b, t).wait_recv()

    def chain_copy(b, t, up_way):
        tile = cols_at(t * COL, COL)
        if up_way:
            spot = jnp.where(b == z + 1, A, b)
            where = (me + B, c)
        else:
            spot, where = b, (me - B, c)
        return remote(
            chain.at[b, :, tile], chain.at[spot, :, tile], c_send, c_recv.at[spot, t], where
        )

    def chain_arrives(spot, t):
        at = chain.at[spot, :, cols_at(t * COL, COL)]
        remote(at, at, c_send, c_recv.at[spot, t], partner).wait_recv()

    def pass_tile(b, t, up_way):
        tile = cols_at(t * COL, COL)
        all_back(b, t)
        mine = contract_rows(place[b], back[b, :, tile])
        fed = (z > 0) if up_way else (z < A - 1)

        @pl.when(fed)
        def _():
            chain_arrives(b, t)
            chain[b, :, tile] = (mine + chain[b, :, tile].astype(f32)).astype(bf16)

        @pl.when(jnp.logical_not(fed))
        def _():
            chain[b, :, tile] = mine.astype(bf16)

        chain_copy(b, t, up_way).start()

    def pass_on(b, up_way):
        @pl.loop(0, tiles)
        def _(t):
            pass_tile(b, t, up_way)

    def settle():
        pairs = ((tokens, tokens_out), (cots, cots_out), (hid, hid_out), (dgate, dgate_out), (dup, dup_out))
        for a, (src, dst) in enumerate(pairs):
            pltpu.make_async_copy(src, dst, out_sem.at[a]).wait()
        for a in range(2):
            sent = rows[a].at[:, pl.ds(0, (B - 1) * cap), :]
            remote(sent, sent, p_send.at[a], p_recv.at[a, 0, 0], partner).wait_send()
            sent = inbox[a].at[:, cols]
            remote(sent, sent, f_send.at[a], f_recv.at[a, 0], partner).wait_send()

        @pl.loop(0, A)
        def _(b):
            for a in range(3):
                whole = meta_all.at[b] if a == 2 else stores[a].at[b]

                @pl.when((b <= z) & (z < A - 1))
                def _():
                    remote(whole, whole, z_up.at[a, b], z_recv.at[a, 0, b], partner).wait_send()

                @pl.when((b >= z) & (z > 0))
                def _():
                    remote(whole, whole, z_dn.at[a, b], z_recv.at[a, 0, b], partner).wait_send()

    at_end = (z == 0) | (z == A - 1)

    find_slots(z)
    for a in range(2):
        for h in range(HALVES):
            pick(a, h, z)
    for load in loads[2:]:
        load.wait()

    def receive(r, h):
        arrive(r, h)

        for side in sides:
            valid, tok, b = side(r)

            @pl.when(valid & tok & (h == HALVES - 1))
            def _():
                find_slots(b)
                for piece_h in range(HALVES):
                    pick(0, piece_h, b)

            @pl.when(valid & jnp.logical_not(tok))
            def _():
                pick(1, h, b)

    run_step = jnp.where(at_end, 0, HALVES - 1)
    lag = jnp.where(at_end, 1, 2)

    def step_of(u, before):
        r, h = lax.div(u, HALVES), lax.rem(u, HALVES)
        receive(r, h)

        @pl.when((r == 1) & (h == 0))
        def _():
            take_in(0, z)
            run_forward(z)

        @pl.when((r == 2) & (h == HALVES - 1 - run_step))
        def _():
            take_in(1, z)
            run_backward(z, -1)

        for side in sides:
            valid, tok, b = side(r - lag)
            now = valid & (h == run_step)

            @pl.when(now & tok)
            def _():
                take_in(0, b)
                run_forward(b)

            @pl.when(now & jnp.logical_not(tok))
            def _():
                take_in(1, b)

        for side in sides:
            valid, tok, b = side(r - lag)
            now = valid & jnp.logical_not(tok) & (h == run_step)

            @pl.when(now)
            def _():
                run_backward(b, before)

            before = jnp.where(now, b, before)

        for up_way, side in ((False, from_below), (True, from_above)):
            valid, tok, b = side(r - 1)

            @pl.when(at_end & valid & jnp.logical_not(tok) & (h == HALVES - 1))
            def _():
                pass_on(b, up_way)

        return before

    last = lax.fori_loop(HALVES, 2 * A * HALVES, step_of, z)

    settle()

    @pl.when(jnp.logical_not(at_end))
    def _():
        @pl.loop(0, A - 1)
        def _(m):
            @pl.loop(0, tiles)
            def _(t):
                @pl.when((above_count <= z) & (m < z))
                def _():
                    pass_tile(m, t, False)

                @pl.when(A - 1 - m > z)
                def _():
                    pass_tile(A - 1 - m, t, True)

                @pl.when((above_count > z) & (m < z))
                def _():
                    pass_tile(m, t, False)

    inner[0] = jnp.zeros((R, 128), f32)

    @pl.loop(0, tiles)
    def _(t):
        tile = cols_at(t * COL, COL)
        all_back(z, t)
        dn[:, tile] = contract_rows(place[z], back[z, :, tile])

        @pl.when(z < A - 1)
        def _():
            chain_arrives(z, t)
            dn[:, tile] += chain[z, :, tile].astype(f32)

        @pl.when(z > 0)
        def _():
            chain_arrives(A, t)
            dn[:, tile] += chain[A, :, tile].astype(f32)

        g_dn = gain[:, tile] * dn[:, tile]
        dn[:, tile] = g_dn
        summed = jnp.sum(mid_all[z, :, tile].astype(f32) * g_dn, axis=1, keepdims=True)
        inner[0] += jnp.broadcast_to(summed, (R, 128))

    share_inner = remote(inner.at[0], inner.at[1], fin.at[0], fin.at[1], partner)
    share_inner.start()
    inv = meta_rows(z)[4]
    eye = lax.broadcasted_iota(jnp.int32, (R, R), 0) == lax.broadcasted_iota(jnp.int32, (R, R), 1)
    inv_tok = jnp.sum(jnp.where(eye, inv, 0.0), axis=1, keepdims=True)
    share_inner.wait()
    drop = inv_tok * inv_tok * inv_tok * ((inner[0, :, 0:1] + inner[1, :, 0:1]) / W)

    @pl.loop(0, tiles)
    def _(t):
        tile = cols_at(t * COL, COL)
        turned = (
            cot_all[z, :, tile].astype(f32)
            + inv_tok * dn[:, tile]
            - mid_all[z, :, tile].astype(f32) * drop
        ).astype(bf16)
        mid_grad[:, tile] = turned
        full[:, cols_at(c * H + t * COL, COL)] = turned

    share_mid = remote(full.at[:, cols], full.at[:, cols], fin.at[2], fin.at[3], partner)
    share_mid.start()

    passed = chain.at[pl.ds(0, A - 1)]
    remote(passed, passed, c_send, c_recv.at[0, 0], partner).wait_send()

    @pl.loop(0, tiles)
    def _(t):
        swap(last, t).wait_send()
        given_to(last, t).wait_send()

    share_mid.wait_send()
    remote(full.at[:, other], full.at[:, other], fin.at[2], fin.at[3], partner).wait_recv()


def experts(mid, cot, ids, prob, first, gain, gate, up, down, n, cap, plane, ident):
    R, H = mid.shape
    F = gate.shape[1]
    W = 2 * H
    B = plane
    A = n // B
    S = B * cap
    anywhere = pl.BlockSpec(memory_space=pl.ANY)
    vmem = pl.BlockSpec(memory_space=pltpu.VMEM)
    dma = pltpu.SemaphoreType.DMA
    tiles = H // COL
    dims = (A, B, cap, R, H, F)
    return pl.pallas_call(
        functools.partial(expert_kernel, dims),
        out_shape=(
            jax.ShapeDtypeStruct((R, H), bf16),
            jax.ShapeDtypeStruct((R, W), bf16),
            jax.ShapeDtypeStruct((A * S, W), bf16),
            jax.ShapeDtypeStruct((A * S, W), bf16),
            jax.ShapeDtypeStruct((A * S, F), bf16),
            jax.ShapeDtypeStruct((A * S, F), bf16),
            jax.ShapeDtypeStruct((A * S, F), bf16),
        ),
        in_specs=[anywhere] * 2 + [vmem] * 4 + [anywhere] * 3,
        out_specs=(vmem, vmem) + (anywhere,) * 5,
        scratch_shapes=[
            pltpu.VMEM((A, R, H), bf16),
            pltpu.VMEM((A, R, H), bf16),
            pltpu.VMEM((A, 2, 8, R), f32),
            pltpu.VMEM((A, S, R), bf16),
            pltpu.VMEM((A, S, 1), f32),
            pltpu.VMEM((A, S, 1), f32),
            pltpu.VMEM((A, S, H), bf16),
            pltpu.VMEM((A, S, H), bf16),
            pltpu.VMEM((A * S, W), bf16),
            pltpu.VMEM((A * S, W), bf16),
            pltpu.VMEM((A * S, F), bf16),
            pltpu.VMEM((A * S, F), bf16),
            pltpu.VMEM((A * S, F), bf16),
            pltpu.VMEM((A * S, F), f32),
            pltpu.VMEM((A * S, F), f32),
            pltpu.VMEM((S, W), bf16),
            pltpu.VMEM((A, S, H), bf16),
            pltpu.VMEM((S, H), bf16),
            pltpu.VMEM((A, S, H), bf16),
            pltpu.VMEM((A + 1, R, H), bf16),
            pltpu.VMEM((R, H), f32),
            pltpu.VMEM((2, R, 128), f32),
            pltpu.VMEM((1, H), f32),
            pltpu.VMEM((W, F), bf16),
            pltpu.VMEM((W, F), bf16),
            pltpu.VMEM((F, W), bf16),
            dma((5,)),
            dma((2,)),
            dma((3, A)),
            dma((3, A)),
            dma((3, HALVES, A)),
            dma((2,)),
            dma((2, HALVES, A)),
            dma((2,)),
            dma((2, A)),
            dma((2, HALVES, A)),
            dma((tiles,)),
            dma((A, tiles)),
            dma((tiles,)),
            dma((A, tiles)),
            dma,
            dma((A + 1, tiles)),
            dma((4,)),
            dma((5,)),
        ],
        compiler_params=pltpu.CompilerParams(
            collective_id=ident, has_side_effects=True, vmem_limit_bytes=VMEM_LIMIT
        ),
        name="experts",
    )(mid, cot, ids, prob, first, gain, gate, up, down)


def combine_kernel(dims, full, normed, out, term, plane_in, line_out, line_in, p_send, p_recv, l_send, l_recv):
    A, B, rows, F = dims
    me, c = lax.axis_index("sp"), lax.axis_index("tp")
    z, q = lax.div(me, B), lax.rem(me, B)
    barrier = pltpu.get_barrier_semaphore()

    @pl.loop(1, B)
    def _(k):
        pl.semaphore_signal(
            barrier, inc=1, device_id=(z * B + lax.rem(q + k, B), c), device_id_type=MESH
        )

    @pl.loop(1, A)
    def _(j):
        pl.semaphore_signal(
            barrier, inc=1, device_id=(lax.rem(z + j, A) * B + q, c), device_id_type=MESH
        )

    def lot(x):
        return pl.ds(pl.multiple_of(x * rows, rows), rows)

    def plane_send(s, k):
        peer = lax.rem(q + k, B)
        return remote(
            term.at[s, lot(peer)], plane_in.at[s, k], p_send.at[s, k], p_recv.at[s, k],
            (z * B + peer, c),
        )

    def line_send(s):
        return remote(
            line_out.at[s], line_in.at[s], l_send.at[s], l_recv.at[s],
            (lax.rem(z + s, A) * B + q, c),
        )

    def product(s):
        block = cols_at(lax.rem(z + s, A) * (B * rows), B * rows)
        got = contract_rows(full[:, block], normed[...])
        term[s] = got.astype(bf16)

    @pl.loop(0, A)
    def _(j):
        s = A - 1 - j
        product(s)

        @pl.when(j == 0)
        def _():
            pl.semaphore_wait(barrier, A + B - 2)

        @pl.loop(1, B)
        def _(k):
            plane_send(s, k).start()

    def plane_sum(s):
        out[...] = term[s, lot(q), :].astype(f32)

        @pl.loop(1, B)
        def _(k):
            plane_send(s, k).wait_recv()
            out[...] += plane_in[s, k].astype(f32)

    @pl.loop(0, A - 1)
    def _(j):
        s = A - 1 - j
        plane_sum(s)
        line_out[s] = out[...].astype(bf16)
        line_send(s).start()

    plane_sum(0)

    @pl.loop(1, A)
    def _(s):
        line_send(s).wait_recv()
        out[...] += line_in[s].astype(f32)

    @pl.loop(0, A)
    def _(s):
        @pl.loop(1, B)
        def _(k):
            plane_send(s, k).wait_send()

        @pl.when(s > 0)
        def _():
            line_send(s).wait_send()


def combine(full, normed, n, plane, ident):
    R, W = full.shape
    F = normed.shape[1]
    A, B = n // plane, plane
    rows = W // n
    vmem = pl.BlockSpec(memory_space=pltpu.VMEM)
    dma = pltpu.SemaphoreType.DMA
    return pl.pallas_call(
        functools.partial(combine_kernel, (A, B, rows, F)),
        out_shape=jax.ShapeDtypeStruct((rows, F), f32),
        in_specs=[vmem, vmem],
        out_specs=vmem,
        scratch_shapes=[
            pltpu.VMEM((A, B * rows, F), bf16),
            pltpu.VMEM((A, B, rows, F), bf16),
            pltpu.VMEM((A, rows, F), bf16),
            pltpu.VMEM((A, rows, F), bf16),
            dma((A, B)),
            dma((A, B)),
            dma((A,)),
            dma((A,)),
        ],
        compiler_params=pltpu.CompilerParams(
            collective_id=ident, has_side_effects=True, vmem_limit_bytes=VMEM_LIMIT
        ),
        name="combine",
    )(full, normed)


def group_mean(values, blocks):
    return jnp.dot(
        values, blocks, precision=lax.Precision.HIGHEST, preferred_element_type=jnp.float32
    ) * (1.0 / GROUP)


def shards(
    mid_stream,
    layer_cot,
    ffn_gain,
    expert_ids,
    group_prob,
    first_share,
    expert_gate,
    expert_up,
    expert_down,
    out_weight,
    conv_gain,
    b_gate,
    c_gate,
    conv_in,
    conv_out,
    conv_taps,
):
    row_count, half_width = mid_stream.shape
    n = lax.axis_size("sp")
    expert_count = n * expert_gate.shape[0]
    slot_count = 4 * row_count // expert_count
    plane = row_count // slot_count
    cap = -(-slot_count // 8) * 8

    gate_w, up_w, down_w = expert_gate[0], expert_up[0], expert_down[0]
    mid_grad, full_mid, tokens_in, cots_in, hidden, d_gate, d_up = experts(
        mid_stream,
        layer_cot,
        expert_ids.T,
        group_prob,
        first_share,
        ffn_gain,
        gate_w,
        up_w,
        down_w,
        n,
        cap,
        plane,
        1,
    )

    channel_count = b_gate.shape[1]
    b32 = b_gate.astype(f32)
    y32 = conv_out.astype(f32)
    gated = b32 * y32
    lane = jnp.arange(channel_count, dtype=jnp.int32) // GROUP
    blocks = (lane[:, None] == lane[None, :]).astype(f32)
    group_rms = lax.rsqrt(group_mean(gated * gated, blocks) + epsilon)
    cgain = conv_gain.astype(f32)[None, :]
    conv_normed = (gated * group_rms * cgain).astype(bf16)

    grad_out_weight = combine(full_mid, conv_normed, n, plane, 2)

    d_normed_conv = jnp.dot(full_mid, out_weight, preferred_element_type=f32)
    g_dc = cgain * d_normed_conv
    group_inner = group_mean(gated * g_dc, blocks)
    d_gated = group_rms * g_dc - gated * (group_rms**3 * group_inner)
    grad_b = (d_gated * y32).astype(bf16)
    d_conv_out = d_gated * b32
    following = from_behind(d_conv_out[:2], "sp", -1)
    grad_down = contract_rows(hidden, cots_in)[None]
    grad_gate = contract_rows(tokens_in, d_gate)[None]
    grad_up = contract_rows(tokens_in, d_up)[None]
    extended = jnp.concatenate([d_conv_out, following], axis=0)
    taps = conv_taps.astype(f32)
    d_mixed = taps[2] * extended[:-2] + taps[1] * extended[1:-1] + taps[0] * extended[2:]
    grad_c = (d_mixed * conv_in.astype(f32)).astype(bf16)
    grad_conv_in = (d_mixed * c_gate.astype(f32)).astype(bf16)
    return (grad_gate, grad_up, grad_down, grad_out_weight, mid_grad, grad_b, grad_c, grad_conv_in)


def solution(mesh):
    placed = (
        P("sp", "tp"),
        P("sp", "tp"),
        P("tp"),
        P("sp", None),
        P("sp"),
        P("sp"),
        P("sp", None, "tp"),
        P("sp", None, "tp"),
        P("sp", "tp", None),
        P(None, "tp"),
        P("tp"),
        P("sp", "tp"),
        P("sp", "tp"),
        P("sp", "tp"),
        P("sp", "tp"),
        P(None, "tp"),
    )
    return jax.shard_map(
        shards,
        mesh=mesh,
        in_specs=placed,
        out_specs=(
            P("sp", None, "tp"),
            P("sp", None, "tp"),
            P("sp", "tp", None),
            P("sp", "tp"),
            P("sp", "tp"),
            P("sp", "tp"),
            P("sp", "tp"),
            P("sp", "tp"),
        ),
        check_vma=False,
    )
```

```python
import functools

import jax
import jax.numpy as jnp
from jax import lax
from jax.experimental import pallas as pl
from jax.experimental.pallas import tpu as pltpu
from jax.sharding import PartitionSpec as P

GROUP = 64
MESH = pl.DeviceIdType.MESH
VMEM_LIMIT = 63 * 1024 * 1024
COL = 256
HALVES = 2

epsilon = 1e-06

f32, bf16 = jnp.float32, jnp.bfloat16


def silu_parts(pre):
    sigma = jax.nn.sigmoid(pre)
    return (pre * sigma, sigma * (1.0 + pre * (1.0 - sigma)))


def contract_rows(left, right):
    return lax.dot_general(
        left, right, (((0,), (0,)), ((), ())), preferred_element_type=jnp.float32
    )


def contract_cols(left, right):
    return lax.dot_general(
        left, right, (((1,), (1,)), ((), ())), preferred_element_type=jnp.float32
    )


def remote(src, dst, send, recv, where):
    return pltpu.make_async_remote_copy(
        src_ref=src,
        dst_ref=dst,
        send_sem=send,
        recv_sem=recv,
        device_id=where,
        device_id_type=MESH,
    )


def cols_at(start, size):
    return pl.ds(pl.multiple_of(start, size), size)


def greet(planes, plane, z, q, c):
    barrier = pltpu.get_barrier_semaphore()
    me = z * plane + q

    def hello(peer, core):
        pl.semaphore_signal(barrier, inc=1, device_id=(peer, core), device_id_type=MESH)

    @pl.loop(1, plane)
    def _(k):
        hello(z * plane + lax.rem(q + k, plane), c)

    hello(me, 1 - c)

    @pl.when(z > 0)
    def _():
        hello(me - plane, c)

    @pl.when(z < planes - 1)
    def _():
        hello(me + plane, c)

    pl.semaphore_wait(barrier, plane + jnp.minimum(z, 1) + jnp.minimum(planes - 1 - z, 1))


def expert_kernel(
    dims,
    mid_in, cot_in, ids, group_prob, first_share, gain_in, gate_in, up_in, down_in,
    mid_grad, full, tokens_out, cots_out, hid_out, dgate_out, dup_out,
    mid_all, cot_all, meta_all, place, inv_col, share_col, rows_tok, rows_cot, tokens, cots,
    hid, dgate, dup, active, slope, part, theirs, total, back, chain, dn, inner, gain,
    gate, up, down,
    ld, meta_sem, z_up, z_dn, z_recv, p_send, p_recv, f_send, f_recv, own_sem,
    x_send, x_recv, b_send, b_recv, c_send, c_recv, fin, out_sem,
):
    A, B, cap, R, H, F = dims
    S, W = B * cap, 2 * H
    tiles = H // COL
    me, c = lax.axis_index("sp"), lax.axis_index("tp")
    z, q = lax.div(me, B), lax.rem(me, B)
    partner = (me, 1 - c)
    cols = cols_at(c * H, H)
    other = cols_at((1 - c) * H, H)

    def slots_of(source):
        return cols_at(source * cap, cap)

    def group_of(b):
        return cols_at(b * S, S)

    above_count = A - 1 - z

    def from_below(r):
        tok = r <= z
        return (r >= 1) & (r <= 2 * z), tok, jnp.where(tok, z - r, r - z - 1)

    def from_above(r):
        tok = r <= above_count
        valid = (r >= 1) & (r <= 2 * above_count)
        return valid, tok, jnp.where(tok, z + r, A + above_count - r)

    sides = (from_below, from_above)

    loads = [
        pltpu.make_async_copy(mid_in, mid_all.at[z], ld.at[0]),
        pltpu.make_async_copy(cot_in, cot_all.at[z], ld.at[1]),
        pltpu.make_async_copy(gate_in, gate, ld.at[2]),
        pltpu.make_async_copy(up_in, up, ld.at[3]),
        pltpu.make_async_copy(down_in, down, ld.at[4]),
    ]
    for load in loads:
        load.start()

    greet(A, B, z, q, c)

    def note_slots():
        crowd = A * B
        row = lax.broadcasted_iota(jnp.int32, (R, R), 0)
        col = lax.broadcasted_iota(jnp.int32, (R, R), 1)
        before = jnp.where(row < col, 1.0, 0.0).astype(bf16)
        expert = lax.broadcasted_iota(jnp.int32, (crowd, R), 0)
        hot = [jnp.where(ids[k : k + 1, :] == expert, 1.0, 0.0) for k in range(2)]
        counted = [jnp.dot(h.astype(bf16), before, preferred_element_type=f32) for h in hot]
        counted[1] = counted[1] + jnp.sum(hot[0], axis=1, keepdims=True)
        squares = jnp.zeros((R, 1), f32)
        for t in range(tiles):
            own = mid_all[z, :, t * COL : (t + 1) * COL].astype(f32)
            squares = squares + jnp.sum(own * own, axis=1, keepdims=True)

        for k in range(2):
            rank = jnp.sum(hot[k] * counted[k], axis=0, keepdims=True)
            meta_all[z, c, k : k + 1, :] = ids[k : k + 1, :].astype(f32) * cap + rank
        prob, first = group_prob[...].reshape(1, R), first_share[...].reshape(1, R)
        meta_all[z, c, 2:3, :] = prob * first
        meta_all[z, c, 3:4, :] = prob * (1.0 - first)
        meta_all[z, c, 4:5, :] = jnp.sum(jnp.where(row == col, squares, 0.0), axis=0, keepdims=True)
        meta_all[z, c, 5:8, :] = jnp.zeros((3, R), f32)
        gain[...] = gain_in[...].astype(f32).reshape(1, H)
        mine = meta_all.at[z, c]
        remote(mine, mine, meta_sem.at[0], meta_sem.at[1], partner).start()
        theirs_at = meta_all.at[z, 1 - c]
        remote(theirs_at, theirs_at, meta_sem.at[0], meta_sem.at[1], partner).wait()

    wide = H // HALVES
    stores = (mid_all, cot_all)

    def piece(h):
        return cols_at(h * wide, wide)

    def z_spot(a, h, b):
        return meta_all.at[b] if a == 2 else stores[a].at[b, :, piece(h)]

    def z_copy(a, h, b, up_way):
        where = (me + B, c) if up_way else (me - B, c)
        sems = z_up if up_way else z_dn
        spot = z_spot(a, h, b)
        return remote(spot, spot, sems.at[a, b], z_recv.at[a, h, b], where)

    def z_own(a, h):
        @pl.when(z < A - 1)
        def _():
            z_copy(a, h, z, True).start()

        @pl.when(z > 0)
        def _():
            z_copy(a, h, z, False).start()

    loads[0].wait()
    for h in range(HALVES):
        z_own(0, h)
    note_slots()
    z_own(2, 0)
    loads[1].wait()

    @pl.when(z == 0)
    def _():
        for h in range(HALVES):
            z_copy(1, h, z, True).start()

    @pl.when(z == A - 1)
    def _():
        for h in range(HALVES):
            z_copy(1, h, z, False).start()

    def landed(a, h, b):
        at = z_spot(a, h, b)
        remote(at, at, z_up.at[a, b], z_recv.at[a, h, b], partner).wait_recv()

    def arrive(r, h):
        for up_way, side in ((True, from_below), (False, from_above)):
            valid, tok, b = side(r)
            onward = (z < A - 1) if up_way else (z > 0)
            last = r == (2 * z if up_way else 2 * above_count)

            @pl.when(valid & tok)
            def _():
                landed(0, h, b)

                @pl.when(onward)
                def _():
                    z_copy(0, h, b, up_way).start()

            @pl.when(valid & tok & (h == HALVES - 1))
            def _():
                landed(2, 0, b)

                @pl.when(onward)
                def _():
                    z_copy(2, 0, b, up_way).start()

            @pl.when(valid & jnp.logical_not(tok))
            def _():
                landed(1, h, b)

                @pl.when(onward)
                def _():
                    z_copy(1, h, b, up_way).start()

            @pl.when(valid & last & onward & (h == HALVES - 1))
            def _():
                for own_h in range(HALVES):
                    z_copy(1, own_h, z, up_way).start()

    rows = (rows_tok, rows_cot)
    inbox = (tokens, cots)

    def in_half(core, h):
        return cols_at(core * H + h * wide, wide)

    def plane_send(a, h, b, k):
        peer = lax.rem(q + k, B)
        return remote(
            rows[a].at[b, slots_of(peer), piece(h)],
            inbox[a].at[slots_of(b * B + q), in_half(c, h)],
            p_send.at[a],
            p_recv.at[a, h, b],
            (z * B + peer, c),
        )

    def plane_landed(a, h, b):
        spot = rows[a].at[b, pl.ds(0, (B - 1) * cap), piece(h)]
        remote(spot, spot, p_send.at[a], p_recv.at[a, h, b], partner).wait_recv()

    def own_local(a, h, b):
        return pltpu.make_async_copy(
            rows[a].at[b, slots_of(q), piece(h)],
            inbox[a].at[slots_of(b * B + q), in_half(c, h)],
            own_sem.at[a, h, b],
        )

    def forward(a, h, b):
        spot = inbox[a].at[group_of(b), in_half(c, h)]
        return remote(spot, spot, f_send.at[a], f_recv.at[a, b], partner)

    def rows_out(a, h, b):
        @pl.loop(1, B)
        def _(k):
            plane_send(a, h, b, k).start()

        own_local(a, h, b).start()

    def meta_rows(b):
        first, second = meta_all[b, 0], meta_all[b, 1]
        inv = lax.rsqrt((first[4:5] + second[4:5]) / W + epsilon)
        base = lax.convert_element_type(z * S, f32)
        return first[0:1] - base, first[1:2] - base, first[2:3], first[3:4], inv

    def find_slots(b):
        slot0, slot1, share0, share1, inv = meta_rows(b)
        slot = lax.broadcasted_iota(jnp.int32, (S, R), 0).astype(f32)
        at0, at1 = slot == slot0, slot == slot1
        hit = at0 | at1
        place[b] = jnp.where(hit, 1.0, 0.0).astype(bf16)
        inv_col[b] = jnp.sum(jnp.where(hit, inv, 0.0), axis=1, keepdims=True)
        share_col[b] = jnp.sum(
            jnp.where(at0, share0, jnp.where(at1, share1, 0.0)), axis=1, keepdims=True
        )

    def pick(a, h, b):
        @pl.loop(0, wide // COL)
        def _(t):
            tile = cols_at(h * wide + t * COL, COL)
            picked = jnp.dot(place[b], stores[a][b, :, tile], preferred_element_type=f32)
            if a == 0:
                rows_tok[b, :, tile] = (picked * inv_col[b] * gain[:, tile]).astype(bf16)
            else:
                rows_cot[b, :, tile] = (picked * share_col[b]).astype(bf16)

        rows_out(a, h, b)

    def swap(b, t):
        tile = cols_at(t * COL, COL)
        return remote(
            part.at[:, cols_at((1 - c) * H + t * COL, COL)],
            theirs.at[b, :, tile],
            x_send.at[t],
            x_recv.at[b, t],
            partner,
        )

    def give_back(b, k, t):
        peer = lax.rem(q + k, B)
        tile = cols_at(t * COL, COL)
        return remote(
            total.at[slots_of(peer), tile],
            back.at[b, slots_of(q), tile],
            b_send.at[t],
            b_recv.at[b, t],
            (z * B + peer, c),
        )

    def given_to(b, t):
        spot = back.at[b, pl.ds(0, (B - 1) * cap), cols_at(t * COL, COL)]
        return remote(spot, spot, b_send.at[t], b_recv.at[b, t], partner)

    def outs_of(b):
        pairs = (
            (tokens, tokens_out), (cots, cots_out), (hid, hid_out), (dgate, dgate_out), (dup, dup_out)
        )
        return [
            pltpu.make_async_copy(src.at[group_of(b)], dst.at[group_of(b)], out_sem.at[a])
            for a, (src, dst) in enumerate(pairs)
        ]

    def take_in(a, b):
        for h in range(HALVES):
            plane_landed(a, h, b)
            own_local(a, h, b).wait()
            forward(a, h, b).start()

    def taken_in(a, b):
        spot = inbox[a].at[group_of(b), other]
        remote(spot, spot, f_send.at[a], f_recv.at[a, b], partner).wait_recv()

    def run_forward(b):
        here = group_of(b)
        taken_in(0, b)

        @pl.loop(0, F // COL)
        def _(t):
            tile = cols_at(t * COL, COL)
            pre_gate = jnp.dot(tokens[here, :], gate[:, tile], preferred_element_type=f32)
            pre_up = jnp.dot(tokens[here, :], up[:, tile], preferred_element_type=f32)
            lit, lean = silu_parts(pre_gate)
            hid[here, tile] = (lit * pre_up).astype(bf16)
            active[here, tile] = lit
            slope[here, tile] = pre_up * lean

    def run_backward(b, before):
        here = group_of(b)
        taken_in(1, b)

        @pl.loop(0, F // COL)
        def _(t):
            tile = cols_at(t * COL, COL)
            d_hidden = contract_cols(cots[here, :], down[tile, :])
            dgate[here, tile] = (d_hidden * slope[here, tile]).astype(bf16)
            dup[here, tile] = (d_hidden * active[here, tile]).astype(bf16)

        for copy in outs_of(b):
            copy.start()

        def part_tile(core, t):
            tile = cols_at(core * H + t * COL, COL)
            got = contract_cols(dgate[here, :], gate[tile, :])
            got = got + contract_cols(dup[here, :], up[tile, :])
            part[:, tile] = got.astype(bf16)

        @pl.loop(0, tiles)
        def _(t):
            @pl.when(before >= 0)
            def _():
                swap(before, t).wait_send()

            part_tile(1 - c, t)
            swap(b, t).start()

        @pl.loop(0, tiles)
        def _(t):
            part_tile(c, t)

            @pl.when(before >= 0)
            def _():
                given_to(b, t).wait_send()

            swap(b, t).wait_recv()
            tile = cols_at(t * COL, COL)
            total[:, tile] = (
                part[:, cols_at(c * H + t * COL, COL)].astype(f32) + theirs[b, :, tile].astype(f32)
            ).astype(bf16)

            @pl.loop(1, B)
            def _(k):
                give_back(b, k, t).start()

            back[b, slots_of(q), tile] = total[slots_of(q), tile]

    def all_back(b, t):
        given_to(b, t).wait_recv()

    def chain_copy(b, t, up_way):
        tile = cols_at(t * COL, COL)
        if up_way:
            spot = jnp.where(b == z + 1, A, b)
            where = (me + B, c)
        else:
            spot, where = b, (me - B, c)
        return remote(
            chain.at[b, :, tile], chain.at[spot, :, tile], c_send, c_recv.at[spot, t], where
        )

    def chain_arrives(spot, t):
        at = chain.at[spot, :, cols_at(t * COL, COL)]
        remote(at, at, c_send, c_recv.at[spot, t], partner).wait_recv()

    def pass_tile(b, t, up_way):
        tile = cols_at(t * COL, COL)
        all_back(b, t)
        mine = contract_rows(place[b], back[b, :, tile])
        fed = (z > 0) if up_way else (z < A - 1)

        @pl.when(fed)
        def _():
            chain_arrives(b, t)
            chain[b, :, tile] = (mine + chain[b, :, tile].astype(f32)).astype(bf16)

        @pl.when(jnp.logical_not(fed))
        def _():
            chain[b, :, tile] = mine.astype(bf16)

        chain_copy(b, t, up_way).start()

    def pass_on(b, up_way):
        @pl.loop(0, tiles)
        def _(t):
            pass_tile(b, t, up_way)

    def settle():
        pairs = ((tokens, tokens_out), (cots, cots_out), (hid, hid_out), (dgate, dgate_out), (dup, dup_out))
        for a, (src, dst) in enumerate(pairs):
            pltpu.make_async_copy(src, dst, out_sem.at[a]).wait()
        for a in range(2):
            sent = rows[a].at[:, pl.ds(0, (B - 1) * cap), :]
            remote(sent, sent, p_send.at[a], p_recv.at[a, 0, 0], partner).wait_send()
            sent = inbox[a].at[:, cols]
            remote(sent, sent, f_send.at[a], f_recv.at[a, 0], partner).wait_send()

        @pl.loop(0, A)
        def _(b):
            for a in range(3):
                whole = meta_all.at[b] if a == 2 else stores[a].at[b]

                @pl.when((b <= z) & (z < A - 1))
                def _():
                    remote(whole, whole, z_up.at[a, b], z_recv.at[a, 0, b], partner).wait_send()

                @pl.when((b >= z) & (z > 0))
                def _():
                    remote(whole, whole, z_dn.at[a, b], z_recv.at[a, 0, b], partner).wait_send()

    at_end = (z == 0) | (z == A - 1)

    find_slots(z)
    for a in range(2):
        for h in range(HALVES):
            pick(a, h, z)
    for load in loads[2:]:
        load.wait()

    def receive(r, h):
        arrive(r, h)

        for side in sides:
            valid, tok, b = side(r)

            @pl.when(valid & tok & (h == HALVES - 1))
            def _():
                find_slots(b)
                for piece_h in range(HALVES):
                    pick(0, piece_h, b)

            @pl.when(valid & jnp.logical_not(tok))
            def _():
                pick(1, h, b)

    run_step = jnp.where(at_end, 0, HALVES - 1)
    lag = jnp.where(at_end, 1, 2)

    def step_of(u, before):
        r, h = lax.div(u, HALVES), lax.rem(u, HALVES)
        receive(r, h)

        @pl.when((r == 1) & (h == 0))
        def _():
            take_in(0, z)
            run_forward(z)

        @pl.when((r == 2) & (h == HALVES - 1 - run_step))
        def _():
            take_in(1, z)
            run_backward(z, -1)

        for side in sides:
            valid, tok, b = side(r - lag)
            now = valid & (h == run_step)

            @pl.when(now & tok)
            def _():
                take_in(0, b)
                run_forward(b)

            @pl.when(now & jnp.logical_not(tok))
            def _():
                take_in(1, b)

        for side in sides:
            valid, tok, b = side(r - lag)
            now = valid & jnp.logical_not(tok) & (h == run_step)

            @pl.when(now)
            def _():
                run_backward(b, before)

            before = jnp.where(now, b, before)

        for up_way, side in ((False, from_below), (True, from_above)):
            valid, tok, b = side(r - 1)

            @pl.when(at_end & valid & jnp.logical_not(tok) & (h == HALVES - 1))
            def _():
                pass_on(b, up_way)

        return before

    last = lax.fori_loop(HALVES, 2 * A * HALVES, step_of, z)

    settle()

    @pl.when(jnp.logical_not(at_end))
    def _():
        @pl.loop(0, A - 1)
        def _(m):
            @pl.loop(0, tiles)
            def _(t):
                @pl.when((above_count <= z) & (m < z))
                def _():
                    pass_tile(m, t, False)

                @pl.when(A - 1 - m > z)
                def _():
                    pass_tile(A - 1 - m, t, True)

                @pl.when((above_count > z) & (m < z))
                def _():
                    pass_tile(m, t, False)

    inner[0] = jnp.zeros((R, 128), f32)

    @pl.loop(0, tiles)
    def _(t):
        tile = cols_at(t * COL, COL)
        all_back(z, t)
        dn[:, tile] = contract_rows(place[z], back[z, :, tile])

        @pl.when(z < A - 1)
        def _():
            chain_arrives(z, t)
            dn[:, tile] += chain[z, :, tile].astype(f32)

        @pl.when(z > 0)
        def _():
            chain_arrives(A, t)
            dn[:, tile] += chain[A, :, tile].astype(f32)

        g_dn = gain[:, tile] * dn[:, tile]
        dn[:, tile] = g_dn
        summed = jnp.sum(mid_all[z, :, tile].astype(f32) * g_dn, axis=1, keepdims=True)
        inner[0] += jnp.broadcast_to(summed, (R, 128))

    share_inner = remote(inner.at[0], inner.at[1], fin.at[0], fin.at[1], partner)
    share_inner.start()
    inv = meta_rows(z)[4]
    eye = lax.broadcasted_iota(jnp.int32, (R, R), 0) == lax.broadcasted_iota(jnp.int32, (R, R), 1)
    inv_tok = jnp.sum(jnp.where(eye, inv, 0.0), axis=1, keepdims=True)
    share_inner.wait()
    drop = inv_tok * inv_tok * inv_tok * ((inner[0, :, 0:1] + inner[1, :, 0:1]) / W)

    @pl.loop(0, tiles)
    def _(t):
        tile = cols_at(t * COL, COL)
        turned = (
            cot_all[z, :, tile].astype(f32)
            + inv_tok * dn[:, tile]
            - mid_all[z, :, tile].astype(f32) * drop
        ).astype(bf16)
        mid_grad[:, tile] = turned
        full[:, cols_at(c * H + t * COL, COL)] = turned

    share_mid = remote(full.at[:, cols], full.at[:, cols], fin.at[2], fin.at[3], partner)
    share_mid.start()

    passed = chain.at[pl.ds(0, A - 1)]
    remote(passed, passed, c_send, c_recv.at[0, 0], partner).wait_send()

    @pl.loop(0, tiles)
    def _(t):
        swap(last, t).wait_send()
        given_to(last, t).wait_send()

    share_mid.wait_send()
    remote(full.at[:, other], full.at[:, other], fin.at[2], fin.at[3], partner).wait_recv()


def experts(mid, cot, ids, prob, first, gain, gate, up, down, n, cap, plane, ident):
    R, H = mid.shape
    F = gate.shape[1]
    W = 2 * H
    B = plane
    A = n // B
    S = B * cap
    anywhere = pl.BlockSpec(memory_space=pl.ANY)
    vmem = pl.BlockSpec(memory_space=pltpu.VMEM)
    dma = pltpu.SemaphoreType.DMA
    tiles = H // COL
    dims = (A, B, cap, R, H, F)
    return pl.pallas_call(
        functools.partial(expert_kernel, dims),
        out_shape=(
            jax.ShapeDtypeStruct((R, H), bf16),
            jax.ShapeDtypeStruct((R, W), bf16),
            jax.ShapeDtypeStruct((A * S, W), bf16),
            jax.ShapeDtypeStruct((A * S, W), bf16),
            jax.ShapeDtypeStruct((A * S, F), bf16),
            jax.ShapeDtypeStruct((A * S, F), bf16),
            jax.ShapeDtypeStruct((A * S, F), bf16),
        ),
        in_specs=[anywhere] * 2 + [vmem] * 4 + [anywhere] * 3,
        out_specs=(vmem, vmem) + (anywhere,) * 5,
        scratch_shapes=[
            pltpu.VMEM((A, R, H), bf16),
            pltpu.VMEM((A, R, H), bf16),
            pltpu.VMEM((A, 2, 8, R), f32),
            pltpu.VMEM((A, S, R), bf16),
            pltpu.VMEM((A, S, 1), f32),
            pltpu.VMEM((A, S, 1), f32),
            pltpu.VMEM((A, S, H), bf16),
            pltpu.VMEM((A, S, H), bf16),
            pltpu.VMEM((A * S, W), bf16),
            pltpu.VMEM((A * S, W), bf16),
            pltpu.VMEM((A * S, F), bf16),
            pltpu.VMEM((A * S, F), bf16),
            pltpu.VMEM((A * S, F), bf16),
            pltpu.VMEM((A * S, F), f32),
            pltpu.VMEM((A * S, F), f32),
            pltpu.VMEM((S, W), bf16),
            pltpu.VMEM((A, S, H), bf16),
            pltpu.VMEM((S, H), bf16),
            pltpu.VMEM((A, S, H), bf16),
            pltpu.VMEM((A + 1, R, H), bf16),
            pltpu.VMEM((R, H), f32),
            pltpu.VMEM((2, R, 128), f32),
            pltpu.VMEM((1, H), f32),
            pltpu.VMEM((W, F), bf16),
            pltpu.VMEM((W, F), bf16),
            pltpu.VMEM((F, W), bf16),
            dma((5,)),
            dma((2,)),
            dma((3, A)),
            dma((3, A)),
            dma((3, HALVES, A)),
            dma((2,)),
            dma((2, HALVES, A)),
            dma((2,)),
            dma((2, A)),
            dma((2, HALVES, A)),
            dma((tiles,)),
            dma((A, tiles)),
            dma((tiles,)),
            dma((A, tiles)),
            dma,
            dma((A + 1, tiles)),
            dma((4,)),
            dma((5,)),
        ],
        compiler_params=pltpu.CompilerParams(
            collective_id=ident, has_side_effects=True, vmem_limit_bytes=VMEM_LIMIT
        ),
        name="experts",
    )(mid, cot, ids, prob, first, gain, gate, up, down)


def group_mean(values, blocks):
    total = jnp.zeros(values.shape, f32)
    for _ in range(3):
        part = values.astype(bf16)
        total = total + jnp.dot(part, blocks, preferred_element_type=f32)
        values = values - part.astype(f32)
    return total * (1.0 / GROUP)


def mixer_kernel(
    dims,
    full_in, b_in, y_in, weight_in, c_in, x_in, cgain_in, taps_in,
    grad_weight, grad_b, grad_c, grad_x,
    full, b_gate, y, weight, c_gate, x, gated, rms, scaled, flow, normed,
    term, plane_in, line_out, line_in,
    ld, p_send, p_recv, l_send, l_recv, halo_sem,
):
    A, B, rows, R, F = dims
    n = A * B
    edge = 8
    me, c = lax.axis_index("sp"), lax.axis_index("tp")
    z, q = lax.div(me, B), lax.rem(me, B)
    loads = [
        pltpu.make_async_copy(src, dst, ld.at[k])
        for k, (src, dst) in enumerate(
            ((b_in, b_gate), (y_in, y), (full_in, full), (weight_in, weight), (c_in, c_gate), (x_in, x))
        )
    ]
    for load in loads:
        load.start()
    barrier = pltpu.get_barrier_semaphore()

    def hello(peer):
        pl.semaphore_signal(barrier, inc=1, device_id=(peer, c), device_id_type=MESH)

    @pl.loop(1, B)
    def _(k):
        hello(z * B + lax.rem(q + k, B))

    @pl.loop(1, A)
    def _(j):
        hello(lax.rem(z + j, A) * B + q)

    apart_before = (q == 0) & (z > 0)
    apart_after = (q == B - 1) & (z < A - 1)

    @pl.when(apart_before)
    def _():
        hello(me - 1)

    @pl.when(apart_after)
    def _():
        hello(me + 1)

    def lot(k):
        return pl.ds(pl.multiple_of(k * rows, rows), rows)

    def plane_send(s, k):
        peer = lax.rem(q + k, B)
        return remote(
            term.at[s, lot(peer)], plane_in.at[s, k], p_send.at[s], p_recv.at[s, k], (z * B + peer, c)
        )

    def line_send(s):
        return remote(
            line_out.at[s], line_in.at[s], l_send.at[s], l_recv.at[s],
            (lax.rem(z + s, A) * B + q, c),
        )

    lane = lax.broadcasted_iota(jnp.int32, (F, F), 0) // GROUP
    blocks = jnp.where(lane == lax.broadcasted_iota(jnp.int32, (F, F), 1) // GROUP, 1.0, 0.0)
    blocks = blocks.astype(bf16)
    cgain = cgain_in[...].astype(f32).reshape(1, F)
    loads[0].wait()
    loads[1].wait()
    gated[...] = b_gate[...].astype(f32) * y[...].astype(f32)
    rms[...] = lax.rsqrt(group_mean(gated[...] * gated[...], blocks) + epsilon)
    normed[...] = (gated[...] * rms[...] * cgain).astype(bf16)
    loads[2].wait()

    @pl.loop(0, A)
    def _(j):
        s = A - 1 - j
        block = cols_at(lax.rem(z + s, A) * (B * rows), B * rows)
        term[s] = contract_rows(full[:, block], normed[...]).astype(bf16)

        @pl.when(j == 0)
        def _():
            pl.semaphore_wait(
                barrier, A + B - 2 + jnp.where(apart_before, 1, 0) + jnp.where(apart_after, 1, 0)
            )

        @pl.loop(1, B)
        def _(k):
            plane_send(s, k).start()

    loads[3].wait()
    scaled[...] = cgain * jnp.dot(full[...], weight[...], preferred_element_type=f32)
    inner = group_mean(gated[...] * scaled[...], blocks)
    d_gated = rms[...] * scaled[...] - gated[...] * (rms[...] * rms[...] * rms[...] * inner)
    grad_b[...] = (d_gated * y[...].astype(f32)).astype(bf16)
    flow[0:R, :] = d_gated * b_gate[...].astype(f32)
    head, tail = flow.at[pl.ds(0, edge)], flow.at[pl.ds(R, edge)]
    to_before = remote(head, tail, halo_sem.at[0], halo_sem.at[1], (me - 1, c))

    @pl.when(me > 0)
    def _():
        to_before.start()

    @pl.when(me == n - 1)
    def _():
        flow[R : R + edge, :] = jnp.zeros((edge, F), f32)

    def plane_sum(s):
        grad_weight[...] = term[s, lot(q), :].astype(f32)

        @pl.loop(1, B)
        def _(k):
            plane_send(s, k).wait_recv()
            grad_weight[...] += plane_in[s, k].astype(f32)

    @pl.loop(0, A - 1)
    def _(j):
        s = A - 1 - j
        plane_sum(s)
        line_out[s] = grad_weight[...].astype(bf16)
        line_send(s).start()

    plane_sum(0)
    for load in loads[4:]:
        load.wait()

    @pl.when(me < n - 1)
    def _():
        remote(tail, tail, halo_sem.at[0], halo_sem.at[1], (me, 1 - c)).wait_recv()

    taps = taps_in[...].astype(f32)
    d_mixed = (
        taps[2:3] * flow[0:R, :] + taps[1:2] * flow[1 : R + 1, :] + taps[0:1] * flow[2 : R + 2, :]
    )
    grad_c[...] = (d_mixed * x[...].astype(f32)).astype(bf16)
    grad_x[...] = (d_mixed * c_gate[...].astype(f32)).astype(bf16)

    @pl.loop(1, A)
    def _(s):
        line_send(s).wait_recv()
        grad_weight[...] += line_in[s].astype(f32)

    @pl.when(me > 0)
    def _():
        to_before.wait_send()

    @pl.loop(0, A)
    def _(s):
        sent = plane_in.at[s, pl.ds(0, B - 1)]
        remote(sent, sent, p_send.at[s], p_recv.at[s, 1], (me, 1 - c)).wait_send()

        @pl.when(s > 0)
        def _():
            line_send(s).wait_send()


def mixer(full, b_gate, y, weight, c_gate, x, cgain, taps, n, plane, ident):
    R, W = full.shape
    F = b_gate.shape[1]
    A, B = n // plane, plane
    rows = W // n
    anywhere = pl.BlockSpec(memory_space=pl.ANY)
    vmem = pl.BlockSpec(memory_space=pltpu.VMEM)
    dma = pltpu.SemaphoreType.DMA
    return pl.pallas_call(
        functools.partial(mixer_kernel, (A, B, rows, R, F)),
        out_shape=(
            jax.ShapeDtypeStruct((rows, F), f32),
            jax.ShapeDtypeStruct((R, F), bf16),
            jax.ShapeDtypeStruct((R, F), bf16),
            jax.ShapeDtypeStruct((R, F), bf16),
        ),
        in_specs=[anywhere] * 6 + [vmem] * 2,
        out_specs=(vmem,) * 4,
        scratch_shapes=[
            pltpu.VMEM((R, W), bf16),
            pltpu.VMEM((R, F), bf16),
            pltpu.VMEM((R, F), bf16),
            pltpu.VMEM((W, F), bf16),
            pltpu.VMEM((R, F), bf16),
            pltpu.VMEM((R, F), bf16),
            pltpu.VMEM((R, F), f32),
            pltpu.VMEM((R, F), f32),
            pltpu.VMEM((R, F), f32),
            pltpu.VMEM((R + 8, F), f32),
            pltpu.VMEM((R, F), bf16),
            pltpu.VMEM((A, B * rows, F), bf16),
            pltpu.VMEM((A, B, rows, F), bf16),
            pltpu.VMEM((A, rows, F), bf16),
            pltpu.VMEM((A, rows, F), bf16),
            dma((6,)),
            dma((A,)),
            dma((A, B)),
            dma((A,)),
            dma((A,)),
            dma((2,)),
        ],
        compiler_params=pltpu.CompilerParams(
            collective_id=ident, has_side_effects=True, vmem_limit_bytes=VMEM_LIMIT
        ),
        name="mixer",
    )(full, b_gate, y, weight, c_gate, x, cgain, taps)


def shards(
    mid_stream,
    layer_cot,
    ffn_gain,
    expert_ids,
    group_prob,
    first_share,
    expert_gate,
    expert_up,
    expert_down,
    out_weight,
    conv_gain,
    b_gate,
    c_gate,
    conv_in,
    conv_out,
    conv_taps,
):
    row_count, half_width = mid_stream.shape
    n = lax.axis_size("sp")
    expert_count = n * expert_gate.shape[0]
    slot_count = 4 * row_count // expert_count
    plane = row_count // slot_count
    cap = -(-slot_count // 8) * 8

    gate_w, up_w, down_w = expert_gate[0], expert_up[0], expert_down[0]
    mid_grad, full_mid, tokens_in, cots_in, hidden, d_gate, d_up = experts(
        mid_stream,
        layer_cot,
        expert_ids.T,
        group_prob,
        first_share,
        ffn_gain,
        gate_w,
        up_w,
        down_w,
        n,
        cap,
        plane,
        1,
    )

    grad_out_weight, grad_b, grad_c, grad_conv_in = mixer(
        full_mid, b_gate, conv_out, out_weight, c_gate, conv_in, conv_gain, conv_taps, n, plane, 2
    )
    grad_down = contract_rows(hidden, cots_in)[None]
    grad_gate = contract_rows(tokens_in, d_gate)[None]
    grad_up = contract_rows(tokens_in, d_up)[None]
    return (grad_gate, grad_up, grad_down, grad_out_weight, mid_grad, grad_b, grad_c, grad_conv_in)


def solution(mesh):
    placed = (
        P("sp", "tp"),
        P("sp", "tp"),
        P("tp"),
        P("sp", None),
        P("sp"),
        P("sp"),
        P("sp", None, "tp"),
        P("sp", None, "tp"),
        P("sp", "tp", None),
        P(None, "tp"),
        P("tp"),
        P("sp", "tp"),
        P("sp", "tp"),
        P("sp", "tp"),
        P("sp", "tp"),
        P(None, "tp"),
    )
    return jax.shard_map(
        shards,
        mesh=mesh,
        in_specs=placed,
        out_specs=(
            P("sp", None, "tp"),
            P("sp", None, "tp"),
            P("sp", "tp", None),
            P("sp", "tp"),
            P("sp", "tp"),
            P("sp", "tp"),
            P("sp", "tp"),
            P("sp", "tp"),
        ),
        check_vma=False,
    )
```

```python
import functools

import jax
import jax.numpy as jnp
from jax import lax
from jax.experimental import pallas as pl
from jax.experimental.pallas import tpu as pltpu
from jax.sharding import PartitionSpec as P

GROUP = 64
MESH = pl.DeviceIdType.MESH
VMEM_LIMIT = 63 * 1024 * 1024
COL = 256
HALVES = 2

epsilon = 1e-06

f32, bf16 = jnp.float32, jnp.bfloat16


def silu_parts(pre):
    sigma = jax.nn.sigmoid(pre)
    return (pre * sigma, sigma * (1.0 + pre * (1.0 - sigma)))


def contract_rows(left, right):
    return lax.dot_general(
        left, right, (((0,), (0,)), ((), ())), preferred_element_type=jnp.float32
    )


def contract_cols(left, right):
    return lax.dot_general(
        left, right, (((1,), (1,)), ((), ())), preferred_element_type=jnp.float32
    )


def remote(src, dst, send, recv, where):
    return pltpu.make_async_remote_copy(
        src_ref=src,
        dst_ref=dst,
        send_sem=send,
        recv_sem=recv,
        device_id=where,
        device_id_type=MESH,
    )


def cols_at(start, size):
    return pl.ds(pl.multiple_of(start, size), size)


def greet(planes, plane, z, q, c):
    barrier = pltpu.get_barrier_semaphore()
    me = z * plane + q

    def hello(peer, core):
        pl.semaphore_signal(barrier, inc=1, device_id=(peer, core), device_id_type=MESH)

    @pl.loop(1, plane)
    def _(k):
        hello(z * plane + lax.rem(q + k, plane), c)

    hello(me, 1 - c)

    @pl.when(z > 0)
    def _():
        hello(me - plane, c)

    @pl.when(z < planes - 1)
    def _():
        hello(me + plane, c)

    pl.semaphore_wait(barrier, plane + jnp.minimum(z, 1) + jnp.minimum(planes - 1 - z, 1))


def expert_kernel(
    dims,
    mid_in, cot_in, ids, group_prob, first_share, gain_in, gate_in, up_in, down_in,
    mid_grad, full, tokens_out, cots_out, hid_out, dgate_out, dup_out,
    mid_all, cot_all, meta_all, place, inv_col, share_col, rows_tok, rows_cot, tokens, cots,
    hid, dgate, dup, active, slope, part, theirs, total, back, chain, dn, inner, gain,
    gate, up, down,
    ld, meta_sem, z_up, z_dn, z_recv, p_send, p_recv, f_send, f_recv, own_sem,
    x_send, x_recv, b_send, b_recv, c_send, c_recv, fin, out_sem,
):
    A, B, cap, R, H, F = dims
    S, W = B * cap, 2 * H
    tiles = H // COL
    me, c = lax.axis_index("sp"), lax.axis_index("tp")
    z, q = lax.div(me, B), lax.rem(me, B)
    partner = (me, 1 - c)
    cols = cols_at(c * H, H)
    other = cols_at((1 - c) * H, H)

    def slots_of(source):
        return cols_at(source * cap, cap)

    def group_of(b):
        return cols_at(b * S, S)

    above_count = A - 1 - z

    def from_below(r):
        tok = r <= z
        return (r >= 1) & (r <= 2 * z), tok, jnp.where(tok, z - r, r - z - 1)

    def from_above(r):
        tok = r <= above_count
        valid = (r >= 1) & (r <= 2 * above_count)
        return valid, tok, jnp.where(tok, z + r, A + above_count - r)

    sides = (from_below, from_above)

    loads = [
        pltpu.make_async_copy(mid_in, mid_all.at[z], ld.at[0]),
        pltpu.make_async_copy(cot_in, cot_all.at[z], ld.at[1]),
        pltpu.make_async_copy(gate_in, gate, ld.at[2]),
        pltpu.make_async_copy(up_in, up, ld.at[3]),
        pltpu.make_async_copy(down_in, down, ld.at[4]),
    ]
    for load in loads:
        load.start()

    greet(A, B, z, q, c)

    def note_slots():
        crowd = A * B
        row = lax.broadcasted_iota(jnp.int32, (R, R), 0)
        col = lax.broadcasted_iota(jnp.int32, (R, R), 1)
        before = jnp.where(row < col, 1.0, 0.0).astype(bf16)
        expert = lax.broadcasted_iota(jnp.int32, (crowd, R), 0)
        hot = [jnp.where(ids[k : k + 1, :] == expert, 1.0, 0.0) for k in range(2)]
        counted = [jnp.dot(h.astype(bf16), before, preferred_element_type=f32) for h in hot]
        counted[1] = counted[1] + jnp.sum(hot[0], axis=1, keepdims=True)
        squares = jnp.zeros((R, 1), f32)
        for t in range(tiles):
            own = mid_all[z, :, t * COL : (t + 1) * COL].astype(f32)
            squares = squares + jnp.sum(own * own, axis=1, keepdims=True)

        for k in range(2):
            rank = jnp.sum(hot[k] * counted[k], axis=0, keepdims=True)
            meta_all[z, c, k : k + 1, :] = ids[k : k + 1, :].astype(f32) * cap + rank
        prob, first = group_prob[...].reshape(1, R), first_share[...].reshape(1, R)
        meta_all[z, c, 2:3, :] = prob * first
        meta_all[z, c, 3:4, :] = prob * (1.0 - first)
        meta_all[z, c, 4:5, :] = jnp.sum(jnp.where(row == col, squares, 0.0), axis=0, keepdims=True)
        meta_all[z, c, 5:8, :] = jnp.zeros((3, R), f32)
        gain[...] = gain_in[...].astype(f32).reshape(1, H)
        mine = meta_all.at[z, c]
        remote(mine, mine, meta_sem.at[0], meta_sem.at[1], partner).start()
        theirs_at = meta_all.at[z, 1 - c]
        remote(theirs_at, theirs_at, meta_sem.at[0], meta_sem.at[1], partner).wait()

    wide = H // HALVES
    stores = (mid_all, cot_all)

    def piece(h):
        return cols_at(h * wide, wide)

    def z_spot(a, h, b):
        return meta_all.at[b] if a == 2 else stores[a].at[b, :, piece(h)]

    def z_copy(a, h, b, up_way):
        where = (me + B, c) if up_way else (me - B, c)
        sems = z_up if up_way else z_dn
        spot = z_spot(a, h, b)
        return remote(spot, spot, sems.at[a, b], z_recv.at[a, h, b], where)

    def z_own(a, h):
        @pl.when(z < A - 1)
        def _():
            z_copy(a, h, z, True).start()

        @pl.when(z > 0)
        def _():
            z_copy(a, h, z, False).start()

    loads[0].wait()
    for h in range(HALVES):
        z_own(0, h)
    note_slots()
    z_own(2, 0)
    loads[1].wait()

    @pl.when(z == 0)
    def _():
        for h in range(HALVES):
            z_copy(1, h, z, True).start()

    @pl.when(z == A - 1)
    def _():
        for h in range(HALVES):
            z_copy(1, h, z, False).start()

    def landed(a, h, b):
        at = z_spot(a, h, b)
        remote(at, at, z_up.at[a, b], z_recv.at[a, h, b], partner).wait_recv()

    def arrive(r, h):
        for up_way, side in ((True, from_below), (False, from_above)):
            valid, tok, b = side(r)
            onward = (z < A - 1) if up_way else (z > 0)
            last = r == (2 * z if up_way else 2 * above_count)

            @pl.when(valid & tok)
            def _():
                landed(0, h, b)

                @pl.when(onward)
                def _():
                    z_copy(0, h, b, up_way).start()

            @pl.when(valid & tok & (h == HALVES - 1))
            def _():
                landed(2, 0, b)

                @pl.when(onward)
                def _():
                    z_copy(2, 0, b, up_way).start()

            @pl.when(valid & jnp.logical_not(tok))
            def _():
                landed(1, h, b)

                @pl.when(onward)
                def _():
                    z_copy(1, h, b, up_way).start()

            @pl.when(valid & last & onward & (h == HALVES - 1))
            def _():
                for own_h in range(HALVES):
                    z_copy(1, own_h, z, up_way).start()

    rows = (rows_tok, rows_cot)
    inbox = (tokens, cots)

    def in_half(core, h):
        return cols_at(core * H + h * wide, wide)

    def plane_send(a, h, b, k):
        peer = lax.rem(q + k, B)
        return remote(
            rows[a].at[b, slots_of(peer), piece(h)],
            inbox[a].at[slots_of(b * B + q), in_half(c, h)],
            p_send.at[a],
            p_recv.at[a, h, b],
            (z * B + peer, c),
        )

    def plane_landed(a, h, b):
        spot = rows[a].at[b, pl.ds(0, (B - 1) * cap), piece(h)]
        remote(spot, spot, p_send.at[a], p_recv.at[a, h, b], partner).wait_recv()

    def own_local(a, h, b):
        return pltpu.make_async_copy(
            rows[a].at[b, slots_of(q), piece(h)],
            inbox[a].at[slots_of(b * B + q), in_half(c, h)],
            own_sem.at[a, h, b],
        )

    def forward(a, h, b):
        spot = inbox[a].at[group_of(b), in_half(c, h)]
        return remote(spot, spot, f_send.at[a], f_recv.at[a, b], partner)

    def rows_out(a, h, b):
        @pl.loop(1, B)
        def _(k):
            plane_send(a, h, b, k).start()

        own_local(a, h, b).start()

    def meta_rows(b):
        first, second = meta_all[b, 0], meta_all[b, 1]
        inv = lax.rsqrt((first[4:5] + second[4:5]) / W + epsilon)
        base = lax.convert_element_type(z * S, f32)
        return first[0:1] - base, first[1:2] - base, first[2:3], first[3:4], inv

    def find_slots(b):
        slot0, slot1, share0, share1, inv = meta_rows(b)
        slot = lax.broadcasted_iota(jnp.int32, (S, R), 0).astype(f32)
        at0, at1 = slot == slot0, slot == slot1
        hit = at0 | at1
        place[b] = jnp.where(hit, 1.0, 0.0).astype(bf16)
        inv_col[b] = jnp.sum(jnp.where(hit, inv, 0.0), axis=1, keepdims=True)
        share_col[b] = jnp.sum(
            jnp.where(at0, share0, jnp.where(at1, share1, 0.0)), axis=1, keepdims=True
        )

    def pick(a, h, b):
        @pl.loop(0, wide // COL)
        def _(t):
            tile = cols_at(h * wide + t * COL, COL)
            picked = jnp.dot(place[b], stores[a][b, :, tile], preferred_element_type=f32)
            if a == 0:
                rows_tok[b, :, tile] = (picked * inv_col[b] * gain[:, tile]).astype(bf16)
            else:
                rows_cot[b, :, tile] = (picked * share_col[b]).astype(bf16)

        rows_out(a, h, b)

    def swap(b, t):
        tile = cols_at(t * COL, COL)
        return remote(
            part.at[:, cols_at((1 - c) * H + t * COL, COL)],
            theirs.at[b, :, tile],
            x_send.at[t],
            x_recv.at[b, t],
            partner,
        )

    def give_back(b, k, t):
        peer = lax.rem(q + k, B)
        tile = cols_at(t * COL, COL)
        return remote(
            total.at[slots_of(peer), tile],
            back.at[b, slots_of(q), tile],
            b_send.at[t],
            b_recv.at[b, t],
            (z * B + peer, c),
        )

    def given_to(b, t):
        spot = back.at[b, pl.ds(0, (B - 1) * cap), cols_at(t * COL, COL)]
        return remote(spot, spot, b_send.at[t], b_recv.at[b, t], partner)

    def outs_of(b):
        pairs = (
            (tokens, tokens_out), (cots, cots_out), (hid, hid_out), (dgate, dgate_out), (dup, dup_out)
        )
        return [
            pltpu.make_async_copy(src.at[group_of(b)], dst.at[group_of(b)], out_sem.at[a])
            for a, (src, dst) in enumerate(pairs)
        ]

    def take_in(a, b):
        for h in range(HALVES):
            plane_landed(a, h, b)
            own_local(a, h, b).wait()
            forward(a, h, b).start()

    def taken_in(a, b):
        spot = inbox[a].at[group_of(b), other]
        remote(spot, spot, f_send.at[a], f_recv.at[a, b], partner).wait_recv()

    def run_forward(b):
        here = group_of(b)
        taken_in(0, b)

        @pl.loop(0, F // COL)
        def _(t):
            tile = cols_at(t * COL, COL)
            pre_gate = jnp.dot(tokens[here, :], gate[:, tile], preferred_element_type=f32)
            pre_up = jnp.dot(tokens[here, :], up[:, tile], preferred_element_type=f32)
            lit, lean = silu_parts(pre_gate)
            hid[here, tile] = (lit * pre_up).astype(bf16)
            active[here, tile] = lit
            slope[here, tile] = pre_up * lean

    def run_backward(b, before):
        here = group_of(b)
        taken_in(1, b)

        @pl.loop(0, F // COL)
        def _(t):
            tile = cols_at(t * COL, COL)
            d_hidden = contract_cols(cots[here, :], down[tile, :])
            dgate[here, tile] = (d_hidden * slope[here, tile]).astype(bf16)
            dup[here, tile] = (d_hidden * active[here, tile]).astype(bf16)

        for copy in outs_of(b):
            copy.start()

        def part_tile(core, t):
            tile = cols_at(core * H + t * COL, COL)
            got = contract_cols(dgate[here, :], gate[tile, :])
            got = got + contract_cols(dup[here, :], up[tile, :])
            part[:, tile] = got.astype(bf16)

        @pl.loop(0, tiles)
        def _(t):
            @pl.when(before >= 0)
            def _():
                swap(before, t).wait_send()

            part_tile(1 - c, t)
            swap(b, t).start()

        @pl.loop(0, tiles)
        def _(t):
            part_tile(c, t)

            @pl.when(before >= 0)
            def _():
                given_to(b, t).wait_send()

            swap(b, t).wait_recv()
            tile = cols_at(t * COL, COL)
            total[:, tile] = (
                part[:, cols_at(c * H + t * COL, COL)].astype(f32) + theirs[b, :, tile].astype(f32)
            ).astype(bf16)

            @pl.loop(1, B)
            def _(k):
                give_back(b, k, t).start()

            back[b, slots_of(q), tile] = total[slots_of(q), tile]

    def all_back(b, t):
        given_to(b, t).wait_recv()

    def chain_copy(b, t, up_way):
        tile = cols_at(t * COL, COL)
        if up_way:
            spot = jnp.where(b == z + 1, A, b)
            where = (me + B, c)
        else:
            spot, where = b, (me - B, c)
        return remote(
            chain.at[b, :, tile], chain.at[spot, :, tile], c_send, c_recv.at[spot, t], where
        )

    def chain_arrives(spot, t):
        at = chain.at[spot, :, cols_at(t * COL, COL)]
        remote(at, at, c_send, c_recv.at[spot, t], partner).wait_recv()

    def pass_tile(b, t, up_way):
        tile = cols_at(t * COL, COL)
        all_back(b, t)
        mine = contract_rows(place[b], back[b, :, tile])
        fed = (z > 0) if up_way else (z < A - 1)

        @pl.when(fed)
        def _():
            chain_arrives(b, t)
            chain[b, :, tile] = (mine + chain[b, :, tile].astype(f32)).astype(bf16)

        @pl.when(jnp.logical_not(fed))
        def _():
            chain[b, :, tile] = mine.astype(bf16)

        chain_copy(b, t, up_way).start()

    def pass_on(b, up_way):
        @pl.loop(0, tiles)
        def _(t):
            pass_tile(b, t, up_way)

    def settle():
        pairs = ((tokens, tokens_out), (cots, cots_out), (hid, hid_out), (dgate, dgate_out), (dup, dup_out))
        for a, (src, dst) in enumerate(pairs):
            pltpu.make_async_copy(src, dst, out_sem.at[a]).wait()
        for a in range(2):
            sent = rows[a].at[:, pl.ds(0, (B - 1) * cap), :]
            remote(sent, sent, p_send.at[a], p_recv.at[a, 0, 0], partner).wait_send()
            sent = inbox[a].at[:, cols]
            remote(sent, sent, f_send.at[a], f_recv.at[a, 0], partner).wait_send()

        @pl.loop(0, A)
        def _(b):
            for a in range(3):
                whole = meta_all.at[b] if a == 2 else stores[a].at[b]

                @pl.when((b <= z) & (z < A - 1))
                def _():
                    remote(whole, whole, z_up.at[a, b], z_recv.at[a, 0, b], partner).wait_send()

                @pl.when((b >= z) & (z > 0))
                def _():
                    remote(whole, whole, z_dn.at[a, b], z_recv.at[a, 0, b], partner).wait_send()

    at_end = (z == 0) | (z == A - 1)

    find_slots(z)
    for a in range(2):
        for h in range(HALVES):
            pick(a, h, z)
    for load in loads[2:]:
        load.wait()

    def receive(r, h):
        arrive(r, h)

        for side in sides:
            valid, tok, b = side(r)

            @pl.when(valid & tok & (h == HALVES - 1))
            def _():
                find_slots(b)
                for piece_h in range(HALVES):
                    pick(0, piece_h, b)

            @pl.when(valid & jnp.logical_not(tok))
            def _():
                pick(1, h, b)

    run_step = jnp.where(at_end, 0, HALVES - 1)
    lag = jnp.where(at_end, 1, 2)

    def step_of(u, before):
        r, h = lax.div(u, HALVES), lax.rem(u, HALVES)
        receive(r, h)

        @pl.when((r == 1) & (h == 0))
        def _():
            take_in(0, z)
            run_forward(z)

        @pl.when((r == 2) & (h == HALVES - 1 - run_step))
        def _():
            take_in(1, z)
            run_backward(z, -1)

        for side in sides:
            valid, tok, b = side(r - lag)
            now = valid & (h == run_step)

            @pl.when(now & tok)
            def _():
                take_in(0, b)
                run_forward(b)

            @pl.when(now & jnp.logical_not(tok))
            def _():
                take_in(1, b)

        for side in sides:
            valid, tok, b = side(r - lag)
            now = valid & jnp.logical_not(tok) & (h == run_step)

            @pl.when(now)
            def _():
                run_backward(b, before)

            before = jnp.where(now, b, before)

        for up_way, side in ((False, from_below), (True, from_above)):
            valid, tok, b = side(r - 1)

            @pl.when(at_end & valid & jnp.logical_not(tok) & (h == HALVES - 1))
            def _():
                pass_on(b, up_way)

        return before

    last = lax.fori_loop(HALVES, 2 * A * HALVES, step_of, z)

    settle()

    @pl.when(jnp.logical_not(at_end))
    def _():
        @pl.loop(0, A - 1)
        def _(m):
            @pl.loop(0, tiles)
            def _(t):
                @pl.when((above_count <= z) & (m < z))
                def _():
                    pass_tile(m, t, False)

                @pl.when(A - 1 - m > z)
                def _():
                    pass_tile(A - 1 - m, t, True)

                @pl.when((above_count > z) & (m < z))
                def _():
                    pass_tile(m, t, False)

    inner[0] = jnp.zeros((R, 128), f32)

    @pl.loop(0, tiles)
    def _(t):
        tile = cols_at(t * COL, COL)
        all_back(z, t)
        dn[:, tile] = contract_rows(place[z], back[z, :, tile])

        @pl.when(z < A - 1)
        def _():
            chain_arrives(z, t)
            dn[:, tile] += chain[z, :, tile].astype(f32)

        @pl.when(z > 0)
        def _():
            chain_arrives(A, t)
            dn[:, tile] += chain[A, :, tile].astype(f32)

        g_dn = gain[:, tile] * dn[:, tile]
        dn[:, tile] = g_dn
        summed = jnp.sum(mid_all[z, :, tile].astype(f32) * g_dn, axis=1, keepdims=True)
        inner[0] += jnp.broadcast_to(summed, (R, 128))

    share_inner = remote(inner.at[0], inner.at[1], fin.at[0], fin.at[1], partner)
    share_inner.start()
    inv = meta_rows(z)[4]
    eye = lax.broadcasted_iota(jnp.int32, (R, R), 0) == lax.broadcasted_iota(jnp.int32, (R, R), 1)
    inv_tok = jnp.sum(jnp.where(eye, inv, 0.0), axis=1, keepdims=True)
    share_inner.wait()
    drop = inv_tok * inv_tok * inv_tok * ((inner[0, :, 0:1] + inner[1, :, 0:1]) / W)

    @pl.loop(0, tiles)
    def _(t):
        tile = cols_at(t * COL, COL)
        turned = (
            cot_all[z, :, tile].astype(f32)
            + inv_tok * dn[:, tile]
            - mid_all[z, :, tile].astype(f32) * drop
        ).astype(bf16)
        mid_grad[:, tile] = turned
        full[:, cols_at(c * H + t * COL, COL)] = turned

    share_mid = remote(full.at[:, cols], full.at[:, cols], fin.at[2], fin.at[3], partner)
    share_mid.start()

    passed = chain.at[pl.ds(0, A - 1)]
    remote(passed, passed, c_send, c_recv.at[0, 0], partner).wait_send()

    @pl.loop(0, tiles)
    def _(t):
        swap(last, t).wait_send()
        given_to(last, t).wait_send()

    share_mid.wait_send()
    remote(full.at[:, other], full.at[:, other], fin.at[2], fin.at[3], partner).wait_recv()


def experts(mid, cot, ids, prob, first, gain, gate, up, down, n, cap, plane, ident):
    R, H = mid.shape
    F = gate.shape[1]
    W = 2 * H
    B = plane
    A = n // B
    S = B * cap
    anywhere = pl.BlockSpec(memory_space=pl.ANY)
    vmem = pl.BlockSpec(memory_space=pltpu.VMEM)
    dma = pltpu.SemaphoreType.DMA
    tiles = H // COL
    dims = (A, B, cap, R, H, F)
    return pl.pallas_call(
        functools.partial(expert_kernel, dims),
        out_shape=(
            jax.ShapeDtypeStruct((R, H), bf16),
            jax.ShapeDtypeStruct((R, W), bf16),
            jax.ShapeDtypeStruct((A * S, W), bf16),
            jax.ShapeDtypeStruct((A * S, W), bf16),
            jax.ShapeDtypeStruct((A * S, F), bf16),
            jax.ShapeDtypeStruct((A * S, F), bf16),
            jax.ShapeDtypeStruct((A * S, F), bf16),
        ),
        in_specs=[anywhere] * 2 + [vmem] * 4 + [anywhere] * 3,
        out_specs=(vmem, vmem) + (anywhere,) * 5,
        scratch_shapes=[
            pltpu.VMEM((A, R, H), bf16),
            pltpu.VMEM((A, R, H), bf16),
            pltpu.VMEM((A, 2, 8, R), f32),
            pltpu.VMEM((A, S, R), bf16),
            pltpu.VMEM((A, S, 1), f32),
            pltpu.VMEM((A, S, 1), f32),
            pltpu.VMEM((A, S, H), bf16),
            pltpu.VMEM((A, S, H), bf16),
            pltpu.VMEM((A * S, W), bf16),
            pltpu.VMEM((A * S, W), bf16),
            pltpu.VMEM((A * S, F), bf16),
            pltpu.VMEM((A * S, F), bf16),
            pltpu.VMEM((A * S, F), bf16),
            pltpu.VMEM((A * S, F), f32),
            pltpu.VMEM((A * S, F), f32),
            pltpu.VMEM((S, W), bf16),
            pltpu.VMEM((A, S, H), bf16),
            pltpu.VMEM((S, H), bf16),
            pltpu.VMEM((A, S, H), bf16),
            pltpu.VMEM((A + 1, R, H), bf16),
            pltpu.VMEM((R, H), f32),
            pltpu.VMEM((2, R, 128), f32),
            pltpu.VMEM((1, H), f32),
            pltpu.VMEM((W, F), bf16),
            pltpu.VMEM((W, F), bf16),
            pltpu.VMEM((F, W), bf16),
            dma((5,)),
            dma((2,)),
            dma((3, A)),
            dma((3, A)),
            dma((3, HALVES, A)),
            dma((2,)),
            dma((2, HALVES, A)),
            dma((2,)),
            dma((2, A)),
            dma((2, HALVES, A)),
            dma((tiles,)),
            dma((A, tiles)),
            dma((tiles,)),
            dma((A, tiles)),
            dma,
            dma((A + 1, tiles)),
            dma((4,)),
            dma((5,)),
        ],
        compiler_params=pltpu.CompilerParams(
            collective_id=ident, has_side_effects=True, vmem_limit_bytes=VMEM_LIMIT
        ),
        name="experts",
    )(mid, cot, ids, prob, first, gain, gate, up, down)


def group_mean(values, blocks):
    total = jnp.zeros(values.shape, f32)
    for _ in range(3):
        part = values.astype(bf16)
        total = total + jnp.dot(part, blocks, preferred_element_type=f32)
        values = values - part.astype(f32)
    return total * (1.0 / GROUP)


def mixer_kernel(
    dims,
    full_in, b_in, y_in, weight_in, c_in, x_in, tokens_in, cots_in, hid_in, dgate_in, dup_in,
    cgain_in, taps_in,
    grad_weight, grad_b, grad_c, grad_x, grad_gate, grad_up, grad_down,
    full, b_gate, y, weight, c_gate, x, gated, rms, scaled, flow, normed,
    term, plane_in, line_out, line_in, tokens, cots, hid, turned, slopes, wide_tile, down_tile,
    ld, p_send, p_recv, l_send, l_recv, halo_sem, tile_sem,
):
    A, B, rows, R, F = dims
    width = full.shape[1]
    fills = width // COL
    n = A * B
    edge = 8
    me, c = lax.axis_index("sp"), lax.axis_index("tp")
    z, q = lax.div(me, B), lax.rem(me, B)
    loads = [
        pltpu.make_async_copy(src, dst, ld.at[k])
        for k, (src, dst) in enumerate(
            (
                (b_in, b_gate),
                (y_in, y),
                (full_in, full),
                (weight_in, weight),
                (c_in, c_gate),
                (x_in, x),
                (hid_in, hid),
                (tokens_in, tokens),
                (dgate_in, slopes.at[:, pl.ds(0, F)]),
                (dup_in, slopes.at[:, pl.ds(F, F)]),
                (cots_in, cots),
            )
        )
    ]
    for load in loads:
        load.start()
    barrier = pltpu.get_barrier_semaphore()

    def hello(peer):
        pl.semaphore_signal(barrier, inc=1, device_id=(peer, c), device_id_type=MESH)

    @pl.loop(1, B)
    def _(k):
        hello(z * B + lax.rem(q + k, B))

    @pl.loop(1, A)
    def _(j):
        hello(lax.rem(z + j, A) * B + q)

    apart_before = (q == 0) & (z > 0)
    apart_after = (q == B - 1) & (z < A - 1)

    @pl.when(apart_before)
    def _():
        hello(me - 1)

    @pl.when(apart_after)
    def _():
        hello(me + 1)

    def lot(k):
        return pl.ds(pl.multiple_of(k * rows, rows), rows)

    def plane_send(s, k):
        peer = lax.rem(q + k, B)
        return remote(
            term.at[s, lot(peer)], plane_in.at[s, k], p_send.at[s], p_recv.at[s, k], (z * B + peer, c)
        )

    def line_send(s):
        return remote(
            line_out.at[s], line_in.at[s], l_send.at[s], l_recv.at[s],
            (lax.rem(z + s, A) * B + q, c),
        )

    lane = lax.broadcasted_iota(jnp.int32, (F, F), 0) // GROUP
    blocks = jnp.where(lane == lax.broadcasted_iota(jnp.int32, (F, F), 1) // GROUP, 1.0, 0.0)
    blocks = blocks.astype(bf16)
    cgain = cgain_in[...].astype(f32).reshape(1, F)
    loads[0].wait()
    loads[1].wait()
    gated[...] = b_gate[...].astype(f32) * y[...].astype(f32)
    rms[...] = lax.rsqrt(group_mean(gated[...] * gated[...], blocks) + epsilon)
    normed[...] = (gated[...] * rms[...] * cgain).astype(bf16)
    loads[2].wait()

    @pl.loop(0, A)
    def _(j):
        s = A - 1 - j
        block = cols_at(lax.rem(z + s, A) * (B * rows), B * rows)
        term[s] = contract_rows(full[:, block], normed[...]).astype(bf16)

        @pl.when(j == 0)
        def _():
            pl.semaphore_wait(
                barrier, A + B - 2 + jnp.where(apart_before, 1, 0) + jnp.where(apart_after, 1, 0)
            )

        @pl.loop(1, B)
        def _(k):
            plane_send(s, k).start()

    loads[3].wait()
    scaled[...] = cgain * jnp.dot(full[...], weight[...], preferred_element_type=f32)
    inner = group_mean(gated[...] * scaled[...], blocks)
    d_gated = rms[...] * scaled[...] - gated[...] * (rms[...] * rms[...] * rms[...] * inner)
    grad_b[...] = (d_gated * y[...].astype(f32)).astype(bf16)
    flow[0:R, :] = d_gated * b_gate[...].astype(f32)
    head, tail = flow.at[pl.ds(0, edge)], flow.at[pl.ds(R, edge)]
    to_before = remote(head, tail, halo_sem.at[0], halo_sem.at[1], (me - 1, c))

    @pl.when(me > 0)
    def _():
        to_before.start()

    @pl.when(me == n - 1)
    def _():
        flow[R : R + edge, :] = jnp.zeros((edge, F), f32)

    def tile_copies(u):
        slot = lax.rem(u, 2)
        at = cols_at(u * COL, COL)
        return (
            pltpu.make_async_copy(wide_tile.at[slot, :, pl.ds(0, F)], grad_gate.at[at], tile_sem.at[0, slot]),
            pltpu.make_async_copy(wide_tile.at[slot, :, pl.ds(F, F)], grad_up.at[at], tile_sem.at[1, slot]),
            pltpu.make_async_copy(down_tile.at[slot], grad_down.at[:, at], tile_sem.at[2, slot]),
        )

    def fill(u):
        slot = lax.rem(u, 2)
        at = cols_at(u * COL, COL)

        @pl.when(u >= 2)
        def _():
            for copy in tile_copies(u - 2):
                copy.wait()

        wide_tile[slot] = contract_rows(tokens[:, at], slopes[...])
        down_tile[slot] = jnp.dot(turned[...], cots[:, at], preferred_element_type=f32)
        for copy in tile_copies(u):
            copy.start()

    per_sum = -(-fills // A)

    def fill_after(j):
        for k in range(per_sum):
            @pl.when(j * per_sum + k < fills)
            def _():
                fill(j * per_sum + k)

    def plane_sum(s):
        grad_weight[...] = term[s, lot(q), :].astype(f32)

        @pl.loop(1, B)
        def _(k):
            plane_send(s, k).wait_recv()
            grad_weight[...] += plane_in[s, k].astype(f32)

    @pl.loop(0, A - 1)
    def _(j):
        s = A - 1 - j
        plane_sum(s)
        line_out[s] = grad_weight[...].astype(bf16)
        line_send(s).start()

        @pl.when(j == 0)
        def _():
            for load in loads[4:]:
                load.wait()
            turned[...] = hid[...].astype(f32).T.astype(bf16)

        fill_after(j)

    plane_sum(0)
    fill_after(A - 1)

    @pl.when(me < n - 1)
    def _():
        remote(tail, tail, halo_sem.at[0], halo_sem.at[1], (me, 1 - c)).wait_recv()

    taps = taps_in[...].astype(f32)
    d_mixed = (
        taps[2:3] * flow[0:R, :] + taps[1:2] * flow[1 : R + 1, :] + taps[0:1] * flow[2 : R + 2, :]
    )
    grad_c[...] = (d_mixed * x[...].astype(f32)).astype(bf16)
    grad_x[...] = (d_mixed * c_gate[...].astype(f32)).astype(bf16)

    @pl.loop(1, A)
    def _(s):
        line_send(s).wait_recv()
        grad_weight[...] += line_in[s].astype(f32)

    @pl.when(me > 0)
    def _():
        to_before.wait_send()

    @pl.loop(0, A)
    def _(s):
        sent = plane_in.at[s, pl.ds(0, B - 1)]
        remote(sent, sent, p_send.at[s], p_recv.at[s, 1], (me, 1 - c)).wait_send()

        @pl.when(s > 0)
        def _():
            line_send(s).wait_send()

    for u in range(max(fills - 2, 0), fills):
        for copy in tile_copies(u):
            copy.wait()


def mixer(full, b_gate, y, weight, c_gate, x, tokens, cots, hid, dgate, dup, cgain, taps, n, plane, ident):
    R, W = full.shape
    F = b_gate.shape[1]
    A, B = n // plane, plane
    rows = W // n
    slots = tokens.shape[0]
    anywhere = pl.BlockSpec(memory_space=pl.ANY)
    vmem = pl.BlockSpec(memory_space=pltpu.VMEM)
    dma = pltpu.SemaphoreType.DMA
    return pl.pallas_call(
        functools.partial(mixer_kernel, (A, B, rows, R, F)),
        out_shape=(
            jax.ShapeDtypeStruct((rows, F), f32),
            jax.ShapeDtypeStruct((R, F), bf16),
            jax.ShapeDtypeStruct((R, F), bf16),
            jax.ShapeDtypeStruct((R, F), bf16),
            jax.ShapeDtypeStruct((W, F), f32),
            jax.ShapeDtypeStruct((W, F), f32),
            jax.ShapeDtypeStruct((F, W), f32),
        ),
        in_specs=[anywhere] * 11 + [vmem] * 2,
        out_specs=(vmem,) * 4 + (anywhere,) * 3,
        scratch_shapes=[
            pltpu.VMEM((R, W), bf16),
            pltpu.VMEM((R, F), bf16),
            pltpu.VMEM((R, F), bf16),
            pltpu.VMEM((W, F), bf16),
            pltpu.VMEM((R, F), bf16),
            pltpu.VMEM((R, F), bf16),
            pltpu.VMEM((R, F), f32),
            pltpu.VMEM((R, F), f32),
            pltpu.VMEM((R, F), f32),
            pltpu.VMEM((R + 8, F), f32),
            pltpu.VMEM((R, F), bf16),
            pltpu.VMEM((A, B * rows, F), bf16),
            pltpu.VMEM((A, B, rows, F), bf16),
            pltpu.VMEM((A, rows, F), bf16),
            pltpu.VMEM((A, rows, F), bf16),
            pltpu.VMEM((slots, W), bf16),
            pltpu.VMEM((slots, W), bf16),
            pltpu.VMEM((slots, F), bf16),
            pltpu.VMEM((F, slots), bf16),
            pltpu.VMEM((slots, 2 * F), bf16),
            pltpu.VMEM((2, COL, 2 * F), f32),
            pltpu.VMEM((2, F, COL), f32),
            dma((11,)),
            dma((A,)),
            dma((A, B)),
            dma((A,)),
            dma((A,)),
            dma((2,)),
            dma((3, 2)),
        ],
        compiler_params=pltpu.CompilerParams(
            collective_id=ident, has_side_effects=True, vmem_limit_bytes=VMEM_LIMIT
        ),
        name="mixer",
    )(full, b_gate, y, weight, c_gate, x, tokens, cots, hid, dgate, dup, cgain, taps)


def shards(
    mid_stream,
    layer_cot,
    ffn_gain,
    expert_ids,
    group_prob,
    first_share,
    expert_gate,
    expert_up,
    expert_down,
    out_weight,
    conv_gain,
    b_gate,
    c_gate,
    conv_in,
    conv_out,
    conv_taps,
):
    row_count, half_width = mid_stream.shape
    n = lax.axis_size("sp")
    expert_count = n * expert_gate.shape[0]
    slot_count = 4 * row_count // expert_count
    plane = row_count // slot_count
    cap = -(-slot_count // 8) * 8

    gate_w, up_w, down_w = expert_gate[0], expert_up[0], expert_down[0]
    mid_grad, full_mid, tokens_in, cots_in, hidden, d_gate, d_up = experts(
        mid_stream,
        layer_cot,
        expert_ids.T,
        group_prob,
        first_share,
        ffn_gain,
        gate_w,
        up_w,
        down_w,
        n,
        cap,
        plane,
        1,
    )

    grad_out_weight, grad_b, grad_c, grad_conv_in, grad_gate, grad_up, grad_down = mixer(
        full_mid,
        b_gate,
        conv_out,
        out_weight,
        c_gate,
        conv_in,
        tokens_in,
        cots_in,
        hidden,
        d_gate,
        d_up,
        conv_gain,
        conv_taps,
        n,
        plane,
        2,
    )
    grad_gate, grad_up, grad_down = grad_gate[None], grad_up[None], grad_down[None]
    return (grad_gate, grad_up, grad_down, grad_out_weight, mid_grad, grad_b, grad_c, grad_conv_in)


def solution(mesh):
    placed = (
        P("sp", "tp"),
        P("sp", "tp"),
        P("tp"),
        P("sp", None),
        P("sp"),
        P("sp"),
        P("sp", None, "tp"),
        P("sp", None, "tp"),
        P("sp", "tp", None),
        P(None, "tp"),
        P("tp"),
        P("sp", "tp"),
        P("sp", "tp"),
        P("sp", "tp"),
        P("sp", "tp"),
        P(None, "tp"),
    )
    return jax.shard_map(
        shards,
        mesh=mesh,
        in_specs=placed,
        out_specs=(
            P("sp", None, "tp"),
            P("sp", None, "tp"),
            P("sp", "tp", None),
            P("sp", "tp"),
            P("sp", "tp"),
            P("sp", "tp"),
            P("sp", "tp"),
            P("sp", "tp"),
        ),
        check_vma=False,
    )
```

```python
import functools

import jax
import jax.numpy as jnp
from jax import lax
from jax.experimental import pallas as pl
from jax.experimental.pallas import tpu as pltpu
from jax.sharding import PartitionSpec as P

GROUP = 64
MESH = pl.DeviceIdType.MESH
VMEM_LIMIT = 63 * 1024 * 1024
COL = 256
HALVES = 4

epsilon = 1e-06

f32, bf16 = jnp.float32, jnp.bfloat16


def silu_parts(pre):
    sigma = jax.nn.sigmoid(pre)
    return (pre * sigma, sigma * (1.0 + pre * (1.0 - sigma)))


def contract_rows(left, right):
    return lax.dot_general(
        left, right, (((0,), (0,)), ((), ())), preferred_element_type=jnp.float32
    )


def contract_cols(left, right):
    return lax.dot_general(
        left, right, (((1,), (1,)), ((), ())), preferred_element_type=jnp.float32
    )


def remote(src, dst, send, recv, where):
    return pltpu.make_async_remote_copy(
        src_ref=src,
        dst_ref=dst,
        send_sem=send,
        recv_sem=recv,
        device_id=where,
        device_id_type=MESH,
    )


def cols_at(start, size):
    return pl.ds(pl.multiple_of(start, size), size)


def greet(planes, plane, z, q, c):
    barrier = pltpu.get_barrier_semaphore()
    me = z * plane + q

    def hello(peer, core):
        pl.semaphore_signal(barrier, inc=1, device_id=(peer, core), device_id_type=MESH)

    @pl.loop(1, plane)
    def _(k):
        hello(z * plane + lax.rem(q + k, plane), c)

    hello(me, 1 - c)

    @pl.when(z > 0)
    def _():
        hello(me - plane, c)

    @pl.when(z < planes - 1)
    def _():
        hello(me + plane, c)

    pl.semaphore_wait(barrier, plane + jnp.minimum(z, 1) + jnp.minimum(planes - 1 - z, 1))


def expert_kernel(
    dims,
    mid_in, cot_in, ids, group_prob, first_share, gain_in, gate_in, up_in, down_in,
    mid_grad, full, tokens_out, cots_out, hid_out, dgate_out, dup_out,
    mid_all, cot_all, meta_all, place, inv_col, share_col, rows_tok, rows_cot, tokens, cots,
    hid, dgate, dup, active, slope, part, theirs, total, back, chain, dn, inner, gain,
    gate, up, down,
    ld, meta_sem, z_up, z_dn, z_recv, p_send, p_recv, f_send, f_recv, own_sem,
    x_send, x_recv, b_send, b_recv, c_send, c_recv, fin, out_sem,
):
    A, B, cap, R, H, F = dims
    S, W = B * cap, 2 * H
    tiles = H // COL
    me, c = lax.axis_index("sp"), lax.axis_index("tp")
    z, q = lax.div(me, B), lax.rem(me, B)
    partner = (me, 1 - c)
    cols = cols_at(c * H, H)
    other = cols_at((1 - c) * H, H)

    def slots_of(source):
        return cols_at(source * cap, cap)

    def group_of(b):
        return cols_at(b * S, S)

    above_count = A - 1 - z

    def from_below(r):
        tok = r <= z
        return (r >= 1) & (r <= 2 * z), tok, jnp.where(tok, z - r, r - z - 1)

    def from_above(r):
        tok = r <= above_count
        valid = (r >= 1) & (r <= 2 * above_count)
        return valid, tok, jnp.where(tok, z + r, A + above_count - r)

    sides = (from_below, from_above)

    loads = [
        pltpu.make_async_copy(mid_in, mid_all.at[z], ld.at[0]),
        pltpu.make_async_copy(cot_in, cot_all.at[z], ld.at[1]),
        pltpu.make_async_copy(gate_in, gate, ld.at[2]),
        pltpu.make_async_copy(up_in, up, ld.at[3]),
        pltpu.make_async_copy(down_in, down, ld.at[4]),
    ]
    for load in loads:
        load.start()

    greet(A, B, z, q, c)

    def note_slots():
        crowd = A * B
        row = lax.broadcasted_iota(jnp.int32, (R, R), 0)
        col = lax.broadcasted_iota(jnp.int32, (R, R), 1)
        before = jnp.where(row < col, 1.0, 0.0).astype(bf16)
        expert = lax.broadcasted_iota(jnp.int32, (crowd, R), 0)
        hot = [jnp.where(ids[k : k + 1, :] == expert, 1.0, 0.0) for k in range(2)]
        counted = [jnp.dot(h.astype(bf16), before, preferred_element_type=f32) for h in hot]
        counted[1] = counted[1] + jnp.sum(hot[0], axis=1, keepdims=True)
        squares = jnp.zeros((R, 1), f32)
        for t in range(tiles):
            own = mid_all[z, :, t * COL : (t + 1) * COL].astype(f32)
            squares = squares + jnp.sum(own * own, axis=1, keepdims=True)

        for k in range(2):
            rank = jnp.sum(hot[k] * counted[k], axis=0, keepdims=True)
            meta_all[z, c, k : k + 1, :] = ids[k : k + 1, :].astype(f32) * cap + rank
        prob, first = group_prob[...].reshape(1, R), first_share[...].reshape(1, R)
        meta_all[z, c, 2:3, :] = prob * first
        meta_all[z, c, 3:4, :] = prob * (1.0 - first)
        meta_all[z, c, 4:5, :] = jnp.sum(jnp.where(row == col, squares, 0.0), axis=0, keepdims=True)
        meta_all[z, c, 5:8, :] = jnp.zeros((3, R), f32)
        gain[...] = gain_in[...].astype(f32).reshape(1, H)
        mine = meta_all.at[z, c]
        remote(mine, mine, meta_sem.at[0], meta_sem.at[1], partner).start()
        theirs_at = meta_all.at[z, 1 - c]
        remote(theirs_at, theirs_at, meta_sem.at[0], meta_sem.at[1], partner).wait()

    wide = H // HALVES
    stores = (mid_all, cot_all)

    def piece(h):
        return cols_at(h * wide, wide)

    def z_spot(a, h, b):
        return meta_all.at[b] if a == 2 else stores[a].at[b, :, piece(h)]

    def z_copy(a, h, b, up_way):
        where = (me + B, c) if up_way else (me - B, c)
        sems = z_up if up_way else z_dn
        spot = z_spot(a, h, b)
        return remote(spot, spot, sems.at[a, b], z_recv.at[a, h, b], where)

    def z_own(a, h):
        @pl.when(z < A - 1)
        def _():
            z_copy(a, h, z, True).start()

        @pl.when(z > 0)
        def _():
            z_copy(a, h, z, False).start()

    loads[0].wait()
    for h in range(HALVES):
        z_own(0, h)
    note_slots()
    z_own(2, 0)
    loads[1].wait()

    @pl.when(z == 0)
    def _():
        for h in range(HALVES):
            z_copy(1, h, z, True).start()

    @pl.when(z == A - 1)
    def _():
        for h in range(HALVES):
            z_copy(1, h, z, False).start()

    def landed(a, h, b):
        at = z_spot(a, h, b)
        remote(at, at, z_up.at[a, b], z_recv.at[a, h, b], partner).wait_recv()

    def arrive(r, h):
        for up_way, side in ((True, from_below), (False, from_above)):
            valid, tok, b = side(r)
            onward = (z < A - 1) if up_way else (z > 0)
            last = r == (2 * z if up_way else 2 * above_count)

            @pl.when(valid & tok)
            def _():
                landed(0, h, b)

                @pl.when(onward)
                def _():
                    z_copy(0, h, b, up_way).start()

            @pl.when(valid & tok & (h == HALVES - 1))
            def _():
                landed(2, 0, b)

                @pl.when(onward)
                def _():
                    z_copy(2, 0, b, up_way).start()

            @pl.when(valid & jnp.logical_not(tok))
            def _():
                landed(1, h, b)

                @pl.when(onward)
                def _():
                    z_copy(1, h, b, up_way).start()

            @pl.when(valid & last & onward & (h == HALVES - 1))
            def _():
                for own_h in range(HALVES):
                    z_copy(1, own_h, z, up_way).start()

    rows = (rows_tok, rows_cot)
    inbox = (tokens, cots)

    def in_half(core, h):
        return cols_at(core * H + h * wide, wide)

    def plane_send(a, h, b, k):
        peer = lax.rem(q + k, B)
        return remote(
            rows[a].at[b, slots_of(peer), piece(h)],
            inbox[a].at[slots_of(b * B + q), in_half(c, h)],
            p_send.at[a],
            p_recv.at[a, h, b],
            (z * B + peer, c),
        )

    def plane_landed(a, h, b):
        spot = rows[a].at[b, pl.ds(0, (B - 1) * cap), piece(h)]
        remote(spot, spot, p_send.at[a], p_recv.at[a, h, b], partner).wait_recv()

    def own_local(a, h, b):
        return pltpu.make_async_copy(
            rows[a].at[b, slots_of(q), piece(h)],
            inbox[a].at[slots_of(b * B + q), in_half(c, h)],
            own_sem.at[a, h, b],
        )

    def forward(a, h, b):
        spot = inbox[a].at[group_of(b), in_half(c, h)]
        return remote(spot, spot, f_send.at[a], f_recv.at[a, b], partner)

    def rows_out(a, h, b):
        @pl.loop(1, B)
        def _(k):
            plane_send(a, h, b, k).start()

        own_local(a, h, b).start()

    def meta_rows(b):
        first, second = meta_all[b, 0], meta_all[b, 1]
        inv = lax.rsqrt((first[4:5] + second[4:5]) / W + epsilon)
        base = lax.convert_element_type(z * S, f32)
        return first[0:1] - base, first[1:2] - base, first[2:3], first[3:4], inv

    def find_slots(b):
        slot0, slot1, share0, share1, inv = meta_rows(b)
        slot = lax.broadcasted_iota(jnp.int32, (S, R), 0).astype(f32)
        at0, at1 = slot == slot0, slot == slot1
        hit = at0 | at1
        place[b] = jnp.where(hit, 1.0, 0.0).astype(bf16)
        inv_col[b] = jnp.sum(jnp.where(hit, inv, 0.0), axis=1, keepdims=True)
        share_col[b] = jnp.sum(
            jnp.where(at0, share0, jnp.where(at1, share1, 0.0)), axis=1, keepdims=True
        )

    def pick(a, h, b):
        @pl.loop(0, wide // COL)
        def _(t):
            tile = cols_at(h * wide + t * COL, COL)
            picked = jnp.dot(place[b], stores[a][b, :, tile], preferred_element_type=f32)
            if a == 0:
                rows_tok[b, :, tile] = (picked * inv_col[b] * gain[:, tile]).astype(bf16)
            else:
                rows_cot[b, :, tile] = (picked * share_col[b]).astype(bf16)

        rows_out(a, h, b)

    def swap(b, t):
        tile = cols_at(t * COL, COL)
        return remote(
            part.at[:, cols_at((1 - c) * H + t * COL, COL)],
            theirs.at[b, :, tile],
            x_send.at[t],
            x_recv.at[b, t],
            partner,
        )

    def give_back(b, k, t):
        peer = lax.rem(q + k, B)
        tile = cols_at(t * COL, COL)
        return remote(
            total.at[slots_of(peer), tile],
            back.at[b, slots_of(q), tile],
            b_send.at[t],
            b_recv.at[b, t],
            (z * B + peer, c),
        )

    def given_to(b, t):
        spot = back.at[b, pl.ds(0, (B - 1) * cap), cols_at(t * COL, COL)]
        return remote(spot, spot, b_send.at[t], b_recv.at[b, t], partner)

    def outs_of(b):
        pairs = (
            (tokens, tokens_out), (cots, cots_out), (hid, hid_out), (dgate, dgate_out), (dup, dup_out)
        )
        return [
            pltpu.make_async_copy(src.at[group_of(b)], dst.at[group_of(b)], out_sem.at[a])
            for a, (src, dst) in enumerate(pairs)
        ]

    def take_in(a, b):
        for h in range(HALVES):
            plane_landed(a, h, b)
            own_local(a, h, b).wait()
            forward(a, h, b).start()

    def taken_in(a, b):
        spot = inbox[a].at[group_of(b), other]
        remote(spot, spot, f_send.at[a], f_recv.at[a, b], partner).wait_recv()

    def run_forward(b):
        here = group_of(b)
        taken_in(0, b)

        @pl.loop(0, F // COL)
        def _(t):
            tile = cols_at(t * COL, COL)
            pre_gate = jnp.dot(tokens[here, :], gate[:, tile], preferred_element_type=f32)
            pre_up = jnp.dot(tokens[here, :], up[:, tile], preferred_element_type=f32)
            lit, lean = silu_parts(pre_gate)
            hid[here, tile] = (lit * pre_up).astype(bf16)
            active[here, tile] = lit
            slope[here, tile] = pre_up * lean

    def run_backward(b, before):
        here = group_of(b)
        taken_in(1, b)

        @pl.loop(0, F // COL)
        def _(t):
            tile = cols_at(t * COL, COL)
            d_hidden = contract_cols(cots[here, :], down[tile, :])
            dgate[here, tile] = (d_hidden * slope[here, tile]).astype(bf16)
            dup[here, tile] = (d_hidden * active[here, tile]).astype(bf16)

        for copy in outs_of(b):
            copy.start()

        def part_tile(core, t):
            tile = cols_at(core * H + t * COL, COL)
            got = contract_cols(dgate[here, :], gate[tile, :])
            got = got + contract_cols(dup[here, :], up[tile, :])
            part[:, tile] = got.astype(bf16)

        @pl.loop(0, tiles)
        def _(t):
            @pl.when(before >= 0)
            def _():
                swap(before, t).wait_send()

            part_tile(1 - c, t)
            swap(b, t).start()

        @pl.loop(0, tiles)
        def _(t):
            part_tile(c, t)

            @pl.when(before >= 0)
            def _():
                given_to(b, t).wait_send()

            swap(b, t).wait_recv()
            tile = cols_at(t * COL, COL)
            total[:, tile] = (
                part[:, cols_at(c * H + t * COL, COL)].astype(f32) + theirs[b, :, tile].astype(f32)
            ).astype(bf16)

            @pl.loop(1, B)
            def _(k):
                give_back(b, k, t).start()

            back[b, slots_of(q), tile] = total[slots_of(q), tile]

    def all_back(b, t):
        given_to(b, t).wait_recv()

    def chain_copy(b, t, up_way):
        tile = cols_at(t * COL, COL)
        if up_way:
            spot = jnp.where(b == z + 1, A, b)
            where = (me + B, c)
        else:
            spot, where = b, (me - B, c)
        return remote(
            chain.at[b, :, tile], chain.at[spot, :, tile], c_send, c_recv.at[spot, t], where
        )

    def chain_arrives(spot, t):
        at = chain.at[spot, :, cols_at(t * COL, COL)]
        remote(at, at, c_send, c_recv.at[spot, t], partner).wait_recv()

    def pass_tile(b, t, up_way):
        tile = cols_at(t * COL, COL)
        all_back(b, t)
        mine = contract_rows(place[b], back[b, :, tile])
        fed = (z > 0) if up_way else (z < A - 1)

        @pl.when(fed)
        def _():
            chain_arrives(b, t)
            chain[b, :, tile] = (mine + chain[b, :, tile].astype(f32)).astype(bf16)

        @pl.when(jnp.logical_not(fed))
        def _():
            chain[b, :, tile] = mine.astype(bf16)

        chain_copy(b, t, up_way).start()

    def pass_on(b, up_way):
        @pl.loop(0, tiles)
        def _(t):
            pass_tile(b, t, up_way)

    def settle():
        pairs = ((tokens, tokens_out), (cots, cots_out), (hid, hid_out), (dgate, dgate_out), (dup, dup_out))
        for a, (src, dst) in enumerate(pairs):
            pltpu.make_async_copy(src, dst, out_sem.at[a]).wait()
        for a in range(2):
            sent = rows[a].at[:, pl.ds(0, (B - 1) * cap), :]
            remote(sent, sent, p_send.at[a], p_recv.at[a, 0, 0], partner).wait_send()
            sent = inbox[a].at[:, cols]
            remote(sent, sent, f_send.at[a], f_recv.at[a, 0], partner).wait_send()

        @pl.loop(0, A)
        def _(b):
            for a in range(3):
                whole = meta_all.at[b] if a == 2 else stores[a].at[b]

                @pl.when((b <= z) & (z < A - 1))
                def _():
                    remote(whole, whole, z_up.at[a, b], z_recv.at[a, 0, b], partner).wait_send()

                @pl.when((b >= z) & (z > 0))
                def _():
                    remote(whole, whole, z_dn.at[a, b], z_recv.at[a, 0, b], partner).wait_send()

    at_end = (z == 0) | (z == A - 1)

    find_slots(z)
    for a in range(2):
        for h in range(HALVES):
            pick(a, h, z)
    for load in loads[2:]:
        load.wait()

    def receive(r, h):
        arrive(r, h)

        for side in sides:
            valid, tok, b = side(r)

            @pl.when(valid & tok & (h == HALVES - 1))
            def _():
                find_slots(b)
                for piece_h in range(HALVES):
                    pick(0, piece_h, b)

            @pl.when(valid & jnp.logical_not(tok))
            def _():
                pick(1, h, b)

    run_step = jnp.where(at_end, 1, HALVES - 1)
    lag = jnp.where(at_end, 1, 2)

    def step_of(u, before):
        r, h = lax.div(u, HALVES), lax.rem(u, HALVES)
        receive(r, h)

        @pl.when((r == 1) & (h == 0))
        def _():
            take_in(0, z)
            run_forward(z)

        @pl.when((r == 2) & (h == jnp.where(at_end, HALVES - 1, 0)))
        def _():
            take_in(1, z)
            run_backward(z, -1)

        for side in sides:
            valid, tok, b = side(r - lag)
            now = valid & (h == run_step)

            @pl.when(now & tok)
            def _():
                take_in(0, b)
                run_forward(b)

            @pl.when(now & jnp.logical_not(tok))
            def _():
                take_in(1, b)

        for side in sides:
            valid, tok, b = side(r - lag)
            now = valid & jnp.logical_not(tok) & (h == run_step)

            @pl.when(now)
            def _():
                run_backward(b, before)

            before = jnp.where(now, b, before)

        for up_way, side in ((False, from_below), (True, from_above)):
            valid, tok, b = side(r - 1)

            @pl.when(at_end & valid & jnp.logical_not(tok) & (h == HALVES - 1))
            def _():
                pass_on(b, up_way)

        return before

    last = lax.fori_loop(HALVES, 2 * A * HALVES, step_of, z)

    settle()

    @pl.when(jnp.logical_not(at_end))
    def _():
        @pl.loop(0, A - 1)
        def _(m):
            @pl.loop(0, tiles)
            def _(t):
                @pl.when((above_count <= z) & (m < z))
                def _():
                    pass_tile(m, t, False)

                @pl.when(A - 1 - m > z)
                def _():
                    pass_tile(A - 1 - m, t, True)

                @pl.when((above_count > z) & (m < z))
                def _():
                    pass_tile(m, t, False)

    inner[0] = jnp.zeros((R, 128), f32)

    @pl.loop(0, tiles)
    def _(t):
        tile = cols_at(t * COL, COL)
        all_back(z, t)
        dn[:, tile] = contract_rows(place[z], back[z, :, tile])

        @pl.when(z < A - 1)
        def _():
            chain_arrives(z, t)
            dn[:, tile] += chain[z, :, tile].astype(f32)

        @pl.when(z > 0)
        def _():
            chain_arrives(A, t)
            dn[:, tile] += chain[A, :, tile].astype(f32)

        g_dn = gain[:, tile] * dn[:, tile]
        dn[:, tile] = g_dn
        summed = jnp.sum(mid_all[z, :, tile].astype(f32) * g_dn, axis=1, keepdims=True)
        inner[0] += jnp.broadcast_to(summed, (R, 128))

    share_inner = remote(inner.at[0], inner.at[1], fin.at[0], fin.at[1], partner)
    share_inner.start()
    inv = meta_rows(z)[4]
    eye = lax.broadcasted_iota(jnp.int32, (R, R), 0) == lax.broadcasted_iota(jnp.int32, (R, R), 1)
    inv_tok = jnp.sum(jnp.where(eye, inv, 0.0), axis=1, keepdims=True)
    share_inner.wait()
    drop = inv_tok * inv_tok * inv_tok * ((inner[0, :, 0:1] + inner[1, :, 0:1]) / W)

    @pl.loop(0, tiles)
    def _(t):
        tile = cols_at(t * COL, COL)
        turned = (
            cot_all[z, :, tile].astype(f32)
            + inv_tok * dn[:, tile]
            - mid_all[z, :, tile].astype(f32) * drop
        ).astype(bf16)
        mid_grad[:, tile] = turned
        full[:, cols_at(c * H + t * COL, COL)] = turned

    share_mid = remote(full.at[:, cols], full.at[:, cols], fin.at[2], fin.at[3], partner)
    share_mid.start()

    passed = chain.at[pl.ds(0, A - 1)]
    remote(passed, passed, c_send, c_recv.at[0, 0], partner).wait_send()

    @pl.loop(0, tiles)
    def _(t):
        swap(last, t).wait_send()
        given_to(last, t).wait_send()

    share_mid.wait_send()
    remote(full.at[:, other], full.at[:, other], fin.at[2], fin.at[3], partner).wait_recv()


def experts(mid, cot, ids, prob, first, gain, gate, up, down, n, cap, plane, ident):
    R, H = mid.shape
    F = gate.shape[1]
    W = 2 * H
    B = plane
    A = n // B
    S = B * cap
    anywhere = pl.BlockSpec(memory_space=pl.ANY)
    vmem = pl.BlockSpec(memory_space=pltpu.VMEM)
    dma = pltpu.SemaphoreType.DMA
    tiles = H // COL
    dims = (A, B, cap, R, H, F)
    return pl.pallas_call(
        functools.partial(expert_kernel, dims),
        out_shape=(
            jax.ShapeDtypeStruct((R, H), bf16),
            jax.ShapeDtypeStruct((R, W), bf16),
            jax.ShapeDtypeStruct((A * S, W), bf16),
            jax.ShapeDtypeStruct((A * S, W), bf16),
            jax.ShapeDtypeStruct((A * S, F), bf16),
            jax.ShapeDtypeStruct((A * S, F), bf16),
            jax.ShapeDtypeStruct((A * S, F), bf16),
        ),
        in_specs=[anywhere] * 2 + [vmem] * 4 + [anywhere] * 3,
        out_specs=(vmem, vmem) + (anywhere,) * 5,
        scratch_shapes=[
            pltpu.VMEM((A, R, H), bf16),
            pltpu.VMEM((A, R, H), bf16),
            pltpu.VMEM((A, 2, 8, R), f32),
            pltpu.VMEM((A, S, R), bf16),
            pltpu.VMEM((A, S, 1), f32),
            pltpu.VMEM((A, S, 1), f32),
            pltpu.VMEM((A, S, H), bf16),
            pltpu.VMEM((A, S, H), bf16),
            pltpu.VMEM((A * S, W), bf16),
            pltpu.VMEM((A * S, W), bf16),
            pltpu.VMEM((A * S, F), bf16),
            pltpu.VMEM((A * S, F), bf16),
            pltpu.VMEM((A * S, F), bf16),
            pltpu.VMEM((A * S, F), f32),
            pltpu.VMEM((A * S, F), f32),
            pltpu.VMEM((S, W), bf16),
            pltpu.VMEM((A, S, H), bf16),
            pltpu.VMEM((S, H), bf16),
            pltpu.VMEM((A, S, H), bf16),
            pltpu.VMEM((A + 1, R, H), bf16),
            pltpu.VMEM((R, H), f32),
            pltpu.VMEM((2, R, 128), f32),
            pltpu.VMEM((1, H), f32),
            pltpu.VMEM((W, F), bf16),
            pltpu.VMEM((W, F), bf16),
            pltpu.VMEM((F, W), bf16),
            dma((5,)),
            dma((2,)),
            dma((3, A)),
            dma((3, A)),
            dma((3, HALVES, A)),
            dma((2,)),
            dma((2, HALVES, A)),
            dma((2,)),
            dma((2, A)),
            dma((2, HALVES, A)),
            dma((tiles,)),
            dma((A, tiles)),
            dma((tiles,)),
            dma((A, tiles)),
            dma,
            dma((A + 1, tiles)),
            dma((4,)),
            dma((5,)),
        ],
        compiler_params=pltpu.CompilerParams(
            collective_id=ident, has_side_effects=True, vmem_limit_bytes=VMEM_LIMIT
        ),
        name="experts",
    )(mid, cot, ids, prob, first, gain, gate, up, down)


def group_mean(values, blocks):
    total = jnp.zeros(values.shape, f32)
    for _ in range(3):
        part = values.astype(bf16)
        total = total + jnp.dot(part, blocks, preferred_element_type=f32)
        values = values - part.astype(f32)
    return total * (1.0 / GROUP)


def mixer_kernel(
    dims,
    full_in, b_in, y_in, weight_in, c_in, x_in, tokens_in, cots_in, hid_in, dgate_in, dup_in,
    cgain_in, taps_in,
    grad_weight, grad_b, grad_c, grad_x, grad_gate, grad_up, grad_down,
    full, b_gate, y, weight, c_gate, x, gated, rms, scaled, flow, normed,
    term, plane_in, line_out, line_in, tokens, cots, hid, turned, slopes, wide_tile, down_tile,
    ld, p_send, p_recv, l_send, l_recv, halo_sem, tile_sem,
):
    A, B, rows, R, F = dims
    width = full.shape[1]
    fills = width // COL
    n = A * B
    edge = 8
    me, c = lax.axis_index("sp"), lax.axis_index("tp")
    z, q = lax.div(me, B), lax.rem(me, B)
    loads = [
        pltpu.make_async_copy(src, dst, ld.at[k])
        for k, (src, dst) in enumerate(
            (
                (b_in, b_gate),
                (y_in, y),
                (full_in, full),
                (weight_in, weight),
                (c_in, c_gate),
                (x_in, x),
                (hid_in, hid),
                (tokens_in, tokens),
                (dgate_in, slopes.at[:, pl.ds(0, F)]),
                (dup_in, slopes.at[:, pl.ds(F, F)]),
                (cots_in, cots),
            )
        )
    ]
    for load in loads:
        load.start()
    barrier = pltpu.get_barrier_semaphore()

    def hello(peer):
        pl.semaphore_signal(barrier, inc=1, device_id=(peer, c), device_id_type=MESH)

    @pl.loop(1, B)
    def _(k):
        hello(z * B + lax.rem(q + k, B))

    @pl.loop(1, A)
    def _(j):
        hello(lax.rem(z + j, A) * B + q)

    apart_before = (q == 0) & (z > 0)
    apart_after = (q == B - 1) & (z < A - 1)

    @pl.when(apart_before)
    def _():
        hello(me - 1)

    @pl.when(apart_after)
    def _():
        hello(me + 1)

    def lot(k):
        return pl.ds(pl.multiple_of(k * rows, rows), rows)

    def plane_send(s, k):
        peer = lax.rem(q + k, B)
        return remote(
            term.at[s, lot(peer)], plane_in.at[s, k], p_send.at[s], p_recv.at[s, k], (z * B + peer, c)
        )

    def line_send(s):
        return remote(
            line_out.at[s], line_in.at[s], l_send.at[s], l_recv.at[s],
            (lax.rem(z + s, A) * B + q, c),
        )

    lane = lax.broadcasted_iota(jnp.int32, (F, F), 0) // GROUP
    blocks = jnp.where(lane == lax.broadcasted_iota(jnp.int32, (F, F), 1) // GROUP, 1.0, 0.0)
    blocks = blocks.astype(bf16)
    cgain = cgain_in[...].astype(f32).reshape(1, F)
    loads[0].wait()
    loads[1].wait()
    gated[...] = b_gate[...].astype(f32) * y[...].astype(f32)
    rms[...] = lax.rsqrt(group_mean(gated[...] * gated[...], blocks) + epsilon)
    normed[...] = (gated[...] * rms[...] * cgain).astype(bf16)
    loads[2].wait()

    @pl.loop(0, A)
    def _(j):
        s = A - 1 - j
        block = cols_at(lax.rem(z + s, A) * (B * rows), B * rows)
        term[s] = contract_rows(full[:, block], normed[...]).astype(bf16)

        @pl.when(j == 0)
        def _():
            pl.semaphore_wait(
                barrier, A + B - 2 + jnp.where(apart_before, 1, 0) + jnp.where(apart_after, 1, 0)
            )

        @pl.loop(1, B)
        def _(k):
            plane_send(s, k).start()

    loads[3].wait()
    scaled[...] = cgain * jnp.dot(full[...], weight[...], preferred_element_type=f32)
    inner = group_mean(gated[...] * scaled[...], blocks)
    d_gated = rms[...] * scaled[...] - gated[...] * (rms[...] * rms[...] * rms[...] * inner)
    grad_b[...] = (d_gated * y[...].astype(f32)).astype(bf16)
    flow[0:R, :] = d_gated * b_gate[...].astype(f32)
    head, tail = flow.at[pl.ds(0, edge)], flow.at[pl.ds(R, edge)]
    to_before = remote(head, tail, halo_sem.at[0], halo_sem.at[1], (me - 1, c))

    @pl.when(me > 0)
    def _():
        to_before.start()

    @pl.when(me == n - 1)
    def _():
        flow[R : R + edge, :] = jnp.zeros((edge, F), f32)

    def tile_copies(u):
        slot = lax.rem(u, 2)
        at = cols_at(u * COL, COL)
        return (
            pltpu.make_async_copy(wide_tile.at[slot, :, pl.ds(0, F)], grad_gate.at[at], tile_sem.at[0, slot]),
            pltpu.make_async_copy(wide_tile.at[slot, :, pl.ds(F, F)], grad_up.at[at], tile_sem.at[1, slot]),
            pltpu.make_async_copy(down_tile.at[slot], grad_down.at[:, at], tile_sem.at[2, slot]),
        )

    def fill(u):
        slot = lax.rem(u, 2)
        at = cols_at(u * COL, COL)

        @pl.when(u >= 2)
        def _():
            for copy in tile_copies(u - 2):
                copy.wait()

        wide_tile[slot] = contract_rows(tokens[:, at], slopes[...])
        down_tile[slot] = jnp.dot(turned[...], cots[:, at], preferred_element_type=f32)
        for copy in tile_copies(u):
            copy.start()

    per_sum = -(-fills // A)

    def fill_after(j):
        for k in range(per_sum):
            @pl.when(j * per_sum + k < fills)
            def _():
                fill(j * per_sum + k)

    def plane_sum(s):
        grad_weight[...] = term[s, lot(q), :].astype(f32)

        @pl.loop(1, B)
        def _(k):
            plane_send(s, k).wait_recv()
            grad_weight[...] += plane_in[s, k].astype(f32)

    @pl.loop(0, A - 1)
    def _(j):
        s = A - 1 - j
        plane_sum(s)
        line_out[s] = grad_weight[...].astype(bf16)
        line_send(s).start()

        @pl.when(j == 0)
        def _():
            for load in loads[4:]:
                load.wait()
            turned[...] = hid[...].astype(f32).T.astype(bf16)

        fill_after(j)

    plane_sum(0)
    fill_after(A - 1)

    @pl.when(me < n - 1)
    def _():
        remote(tail, tail, halo_sem.at[0], halo_sem.at[1], (me, 1 - c)).wait_recv()

    taps = taps_in[...].astype(f32)
    d_mixed = (
        taps[2:3] * flow[0:R, :] + taps[1:2] * flow[1 : R + 1, :] + taps[0:1] * flow[2 : R + 2, :]
    )
    grad_c[...] = (d_mixed * x[...].astype(f32)).astype(bf16)
    grad_x[...] = (d_mixed * c_gate[...].astype(f32)).astype(bf16)

    @pl.loop(1, A)
    def _(s):
        line_send(s).wait_recv()
        grad_weight[...] += line_in[s].astype(f32)

    @pl.when(me > 0)
    def _():
        to_before.wait_send()

    @pl.loop(0, A)
    def _(s):
        sent = plane_in.at[s, pl.ds(0, B - 1)]
        remote(sent, sent, p_send.at[s], p_recv.at[s, 1], (me, 1 - c)).wait_send()

        @pl.when(s > 0)
        def _():
            line_send(s).wait_send()

    for u in range(max(fills - 2, 0), fills):
        for copy in tile_copies(u):
            copy.wait()


def mixer(full, b_gate, y, weight, c_gate, x, tokens, cots, hid, dgate, dup, cgain, taps, n, plane, ident):
    R, W = full.shape
    F = b_gate.shape[1]
    A, B = n // plane, plane
    rows = W // n
    slots = tokens.shape[0]
    anywhere = pl.BlockSpec(memory_space=pl.ANY)
    vmem = pl.BlockSpec(memory_space=pltpu.VMEM)
    dma = pltpu.SemaphoreType.DMA
    return pl.pallas_call(
        functools.partial(mixer_kernel, (A, B, rows, R, F)),
        out_shape=(
            jax.ShapeDtypeStruct((rows, F), f32),
            jax.ShapeDtypeStruct((R, F), bf16),
            jax.ShapeDtypeStruct((R, F), bf16),
            jax.ShapeDtypeStruct((R, F), bf16),
            jax.ShapeDtypeStruct((W, F), f32),
            jax.ShapeDtypeStruct((W, F), f32),
            jax.ShapeDtypeStruct((F, W), f32),
        ),
        in_specs=[anywhere] * 11 + [vmem] * 2,
        out_specs=(vmem,) * 4 + (anywhere,) * 3,
        scratch_shapes=[
            pltpu.VMEM((R, W), bf16),
            pltpu.VMEM((R, F), bf16),
            pltpu.VMEM((R, F), bf16),
            pltpu.VMEM((W, F), bf16),
            pltpu.VMEM((R, F), bf16),
            pltpu.VMEM((R, F), bf16),
            pltpu.VMEM((R, F), f32),
            pltpu.VMEM((R, F), f32),
            pltpu.VMEM((R, F), f32),
            pltpu.VMEM((R + 8, F), f32),
            pltpu.VMEM((R, F), bf16),
            pltpu.VMEM((A, B * rows, F), bf16),
            pltpu.VMEM((A, B, rows, F), bf16),
            pltpu.VMEM((A, rows, F), bf16),
            pltpu.VMEM((A, rows, F), bf16),
            pltpu.VMEM((slots, W), bf16),
            pltpu.VMEM((slots, W), bf16),
            pltpu.VMEM((slots, F), bf16),
            pltpu.VMEM((F, slots), bf16),
            pltpu.VMEM((slots, 2 * F), bf16),
            pltpu.VMEM((2, COL, 2 * F), f32),
            pltpu.VMEM((2, F, COL), f32),
            dma((11,)),
            dma((A,)),
            dma((A, B)),
            dma((A,)),
            dma((A,)),
            dma((2,)),
            dma((3, 2)),
        ],
        compiler_params=pltpu.CompilerParams(
            collective_id=ident, has_side_effects=True, vmem_limit_bytes=VMEM_LIMIT
        ),
        name="mixer",
    )(full, b_gate, y, weight, c_gate, x, tokens, cots, hid, dgate, dup, cgain, taps)


def shards(
    mid_stream,
    layer_cot,
    ffn_gain,
    expert_ids,
    group_prob,
    first_share,
    expert_gate,
    expert_up,
    expert_down,
    out_weight,
    conv_gain,
    b_gate,
    c_gate,
    conv_in,
    conv_out,
    conv_taps,
):
    row_count, half_width = mid_stream.shape
    n = lax.axis_size("sp")
    expert_count = n * expert_gate.shape[0]
    slot_count = 4 * row_count // expert_count
    plane = row_count // slot_count
    cap = -(-slot_count // 8) * 8

    gate_w, up_w, down_w = expert_gate[0], expert_up[0], expert_down[0]
    mid_grad, full_mid, tokens_in, cots_in, hidden, d_gate, d_up = experts(
        mid_stream,
        layer_cot,
        expert_ids.T,
        group_prob,
        first_share,
        ffn_gain,
        gate_w,
        up_w,
        down_w,
        n,
        cap,
        plane,
        1,
    )

    grad_out_weight, grad_b, grad_c, grad_conv_in, grad_gate, grad_up, grad_down = mixer(
        full_mid,
        b_gate,
        conv_out,
        out_weight,
        c_gate,
        conv_in,
        tokens_in,
        cots_in,
        hidden,
        d_gate,
        d_up,
        conv_gain,
        conv_taps,
        n,
        plane,
        2,
    )
    grad_gate, grad_up, grad_down = grad_gate[None], grad_up[None], grad_down[None]
    return (grad_gate, grad_up, grad_down, grad_out_weight, mid_grad, grad_b, grad_c, grad_conv_in)


def solution(mesh):
    placed = (
        P("sp", "tp"),
        P("sp", "tp"),
        P("tp"),
        P("sp", None),
        P("sp"),
        P("sp"),
        P("sp", None, "tp"),
        P("sp", None, "tp"),
        P("sp", "tp", None),
        P(None, "tp"),
        P("tp"),
        P("sp", "tp"),
        P("sp", "tp"),
        P("sp", "tp"),
        P("sp", "tp"),
        P(None, "tp"),
    )
    return jax.shard_map(
        shards,
        mesh=mesh,
        in_specs=placed,
        out_specs=(
            P("sp", None, "tp"),
            P("sp", None, "tp"),
            P("sp", "tp", None),
            P("sp", "tp"),
            P("sp", "tp"),
            P("sp", "tp"),
            P("sp", "tp"),
            P("sp", "tp"),
        ),
        check_vma=False,
    )
```
